32 devices in a mesh: sp: 8 (over z, x), tp: 4 (over y, core).
Axes of the slice: x: 2, y: 2, z: 4, core: 2. Of those that a mesh axis runs over, the one named last changes fastest.
Arguments:
- tokens: bfloat16 [4096, 2048], P(('sp', 'tp')), may hold values from -6 to 6
- input_norm_scale: bfloat16 [2048], replicated, may hold values from 0.099609375 to 1.8984375
- outer_gate_weight: bfloat16 [2048, 1024], P('sp', 'tp'), may hold values from -0.125 to 0.125
- inner_gate_weight: bfloat16 [2048, 1024], P('sp', 'tp'), may hold values from -0.125 to 0.125
- value_weight_matrix: bfloat16 [2048, 1024], P('sp', 'tp'), may hold values from -0.125 to 0.125
- output_gate_weight: bfloat16 [2048, 1024], P('sp', 'tp'), may hold values from -0.125 to 0.125
- state_input_weight: bfloat16 [2048, 1024], P('sp', 'tp'), may hold values from -0.125 to 0.125
- write_key_weight: bfloat16 [2048, 512], P('sp', 'tp'), may hold values from -0.125 to 0.125
- read_key_weight: bfloat16 [2048, 512], P('sp', 'tp'), may hold values from -0.125 to 0.125
- step_size_weight: bfloat16 [2048, 16], P(None, 'tp'), may hold values from -0.125 to 0.125
- gated_conv_weight: bfloat16 [3, 1024], P(None, 'tp'), may hold values from -3.5 to 3.5
- input_conv_weight: bfloat16 [4, 1024], P(None, 'tp'), may hold values from -3 to 3
- write_conv_weight: bfloat16 [4, 512], P(None, 'tp'), may hold values from -3 to 3
- read_conv_weight: bfloat16 [4, 512], P(None, 'tp'), may hold values from -3 to 3
- step_size_bias: float32 [16], P('tp'), may hold values from -1 to 0.5
- log_decay_rate: float32 [16], P('tp'), may hold values from -16 to -2.5, as said below
- decay_spikes: float32 [16, 4096], P('tp', 'sp'), may hold values from -1 to 0, as said below
- direct_path_weight: float32 [16], P('tp'), may hold values from 0.5 to 2
- head_norm_scale: bfloat16 [1024], P('tp'), may hold values from 0.099609375 to 1.8984375
- conv_output_weight: bfloat16 [1024, 2048], P('tp', 'sp'), may hold values from -0.125 to 0.125
- state_output_weight: bfloat16 [1024, 2048], P('tp', 'sp'), may hold values from -0.125 to 0.125
Outputs:
- mixed: bfloat16 [4096, 2048], P(('sp', 'tp'))
The draws below stay inside these ranges and needn't reach their ends.
Inputs may be any that keep to these rules, and one draw needn't show every extreme that they name: `log_decay_rate`: one value a head. `decay_spikes`: never positive.
All inputs are finite; a program needn't handle non-finite values.
Results may differ from the reference program's by a relative error of at most 0.017.
Values may be sent and summed in bfloat16 or wider, within the bound.
A program may use at most 128 MiB of HBM per device.

```python
import math
import jax
import jax.numpy as jnp
from jax import lax

D = 2048
CONV = 1024
MIXER_HEADS = 16
HEAD_DIM = 64
GROUPS = 4
STATE = 128
SHORT_K = 3
SSD_K = 4
BLOCK = 64
TOK_DEV = 512
INNER = 1024
SEQUENCE_TOKENS = 4096
N_TP = 4


def draw_tokens(key, part):
    positions = jnp.arange(SEQUENCE_TOKENS, dtype=jnp.int32)
    segment_ids = positions * 8 // SEQUENCE_TOKENS
    jitter_values = jax.random.truncated_normal(jax.random.fold_in(key, 31), -4.5, 4.5, (SEQUENCE_TOKENS, D), jnp.float32)
    directions = jax.random.uniform(jax.random.fold_in(key, 32), (8, D), jnp.float32, -1.2, 1.2)
    offsets = jnp.take(directions, segment_ids, axis=0)
    return (jitter_values + offsets).astype(jnp.bfloat16)


def draw_log_decay_rate(key, part):
    ranking = jax.random.permutation(jax.random.fold_in(key, 11), MIXER_HEADS)
    quick_heads = ranking < MIXER_HEADS // 2
    fast_rates = jnp.exp(jax.random.uniform(jax.random.fold_in(key, 12), (MIXER_HEADS,), jnp.float32, math.log(0.02), math.log(0.08)))
    slow_rates = jnp.exp(jax.random.uniform(jax.random.fold_in(key, 13), (MIXER_HEADS,), jnp.float32, math.log(0.1), math.log(0.3))) / SEQUENCE_TOKENS
    return jnp.log(jnp.where(quick_heads, fast_rates, slow_rates)).astype(jnp.float32)


def draw_decay_spikes(key, part):
    blocks = SEQUENCE_TOKENS // TOK_DEV
    levels = jnp.exp(jax.random.uniform(jax.random.fold_in(key, 21), (MIXER_HEADS, blocks), jnp.float32, math.log(0.25), math.log(2.0)))
    stable_decay = -0.3 / SEQUENCE_TOKENS * jnp.repeat(levels, TOK_DEV, axis=1)
    spike_positions = jax.random.randint(jax.random.fold_in(key, 22), (3,), 0, SEQUENCE_TOKENS)
    spike_present = jnp.any(jnp.arange(SEQUENCE_TOKENS)[None, :] == spike_positions[:, None], axis=0)
    spike_decrement = jax.random.uniform(jax.random.fold_in(key, 23), (MIXER_HEADS, SEQUENCE_TOKENS), jnp.float32, 0.22, 0.69)
    return (stable_decay - jnp.where(spike_present[None, :], spike_decrement, 0.0)).astype(jnp.float32)


def steps_of(own_key, dims, pieces, least, largest):
    level, own = 1.0, jax.random.fold_in(own_key, 6)
    for dim, parts in pieces:
        draws = jnp.exp(jax.random.uniform(jax.random.fold_in(own, dim), (parts,), jnp.float32, least / len(pieces), largest / len(pieces)))
        level = level * jnp.repeat(draws, dims[dim] // parts).reshape([-1 if axis == dim else 1 for axis in range(len(dims))])
    return level


def gaussian(rng, shape, deviation, limit, pieces=(), kind=jnp.bfloat16):
    drawn = jax.random.normal(rng, shape, jnp.float32) * deviation
    if len(pieces) > 0:
        drawn = steps_of(rng, shape, pieces, -0.22, 0.18) * drawn
    return jnp.clip(drawn, min=-limit, max=limit).astype(kind)


def setup_inputs(seed: int = 0) -> dict:
    streams_of = jax.random.split(jax.random.key(seed), 22)
    return {
        "tokens": draw_tokens(jax.random.fold_in(streams_of[21], 71), 0),
        "input_norm_scale": jnp.clip(1.0 + 0.18 * jax.random.normal(streams_of[1], (D,), jnp.float32), 0.099609375, 1.8984375).astype(jnp.bfloat16),
        "outer_gate_weight": gaussian(streams_of[2], (D, CONV), D ** -0.5, 0.125, ((0, 8), (1, 4))),
        "inner_gate_weight": gaussian(streams_of[3], (D, CONV), D ** -0.5, 0.125, ((0, 8), (1, 4))),
        "value_weight_matrix": gaussian(streams_of[4], (D, CONV), D ** -0.5, 0.125, ((0, 8), (1, 4))),
        "output_gate_weight": gaussian(streams_of[5], (D, INNER), D ** -0.5, 0.125, ((0, 8), (1, 4))),
        "state_input_weight": gaussian(streams_of[6], (D, INNER), D ** -0.5, 0.125, ((0, 8), (1, 4))),
        "write_key_weight": gaussian(streams_of[7], (D, GROUPS * STATE), D ** -0.5, 0.125, ((0, 8), (1, 4))),
        "read_key_weight": gaussian(streams_of[8], (D, GROUPS * STATE), D ** -0.5, 0.125, ((0, 8), (1, 4))),
        "step_size_weight": gaussian(streams_of[9], (D, MIXER_HEADS), D ** -0.5, 0.125, ((1, 4),)),
        "gated_conv_weight": gaussian(streams_of[10], (SHORT_K, CONV), SHORT_K ** -0.5, 3.5, ((1, 4),)),
        "input_conv_weight": gaussian(streams_of[11], (SSD_K, INNER), SSD_K ** -0.5, 3.0, ((1, 4),)),
        "write_conv_weight": gaussian(streams_of[12], (SSD_K, GROUPS * STATE), SSD_K ** -0.5, 3.0, ((1, 4),)),
        "read_conv_weight": gaussian(streams_of[13], (SSD_K, GROUPS * STATE), SSD_K ** -0.5, 3.0, ((1, 4),)),
        "step_size_bias": jnp.clip(-1.0 + 1.5 * jax.random.uniform(streams_of[14], (MIXER_HEADS,), jnp.float32) ** steps_of(streams_of[14], (MIXER_HEADS,), ((0, 4),), -0.2, 0.2), -1.0, 0.5),
        "log_decay_rate": draw_log_decay_rate(jax.random.fold_in(streams_of[21], 71), 0),
        "decay_spikes": draw_decay_spikes(jax.random.fold_in(streams_of[21], 71), 0),
        "direct_path_weight": jnp.clip(0.5 + 1.5 * jax.random.uniform(streams_of[17], (MIXER_HEADS,), jnp.float32) ** steps_of(streams_of[17], (MIXER_HEADS,), ((0, 4),), -0.2, 0.2), 0.5, 2.0),
        "head_norm_scale": jnp.clip(1.0 + 0.18 * jax.random.normal(streams_of[18], (INNER,), jnp.float32), 0.099609375, 1.8984375).astype(jnp.bfloat16),
        "conv_output_weight": gaussian(streams_of[19], (CONV, D), (CONV + INNER) ** -0.5, 0.125, ((0, 4), (1, 8))),
        "state_output_weight": gaussian(streams_of[20], (INNER, D), (CONV + INNER) ** -0.5, 0.125, ((0, 4), (1, 8))),
    }


epsilon = 1e-05
highest = lax.Precision.HIGHEST

def causal_taps(values, tap_weights):
    tap_count = tap_weights.shape[0]
    length = values.shape[0]
    padded = jnp.concatenate([jnp.zeros((tap_count - 1, values.shape[1]), jnp.float32), values], axis=0)
    running = tap_weights[0] * padded[0:length]
    for offset in range(1, tap_count):
        running = running + tap_weights[offset] * padded[offset:offset + length]
    return running

def reference(tokens, input_norm_scale, outer_gate_weight, inner_gate_weight, value_weight_matrix, output_gate_weight, state_input_weight, write_key_weight, read_key_weight, step_size_weight, gated_conv_weight, input_conv_weight, write_conv_weight, read_conv_weight, step_size_bias, log_decay_rate, decay_spikes, direct_path_weight, head_norm_scale, conv_output_weight, state_output_weight):
    token_rows = tokens.astype(jnp.float32)
    scaled = token_rows * lax.rsqrt(lax.optimization_barrier(jnp.mean(token_rows * token_rows, axis=1, keepdims=True)) + epsilon)
    normed = (scaled * input_norm_scale.astype(jnp.float32)).astype(jnp.bfloat16)

    def project(weight):
        return jnp.dot(normed, weight, preferred_element_type=jnp.float32).astype(jnp.bfloat16)
    outer_gate = project(outer_gate_weight)
    inner_gate = project(inner_gate_weight)
    conv_input = project(value_weight_matrix)
    out_gate = project(output_gate_weight)
    state_input = project(state_input_weight)
    write_keys = project(write_key_weight)
    read_keys = project(read_key_weight)
    step_raw = jnp.dot(normed, step_size_weight, preferred_element_type=jnp.float32)
    product = inner_gate.astype(jnp.float32) * conv_input.astype(jnp.float32)
    mixer_part = (outer_gate.astype(jnp.float32) * causal_taps(product, gated_conv_weight.astype(jnp.float32))).astype(jnp.bfloat16)
    seq_input = jax.nn.silu(causal_taps(state_input.astype(jnp.float32), input_conv_weight.astype(jnp.float32)))
    seq_write = jax.nn.silu(causal_taps(write_keys.astype(jnp.float32), write_conv_weight.astype(jnp.float32)))
    seq_read = jax.nn.silu(causal_taps(read_keys.astype(jnp.float32), read_conv_weight.astype(jnp.float32)))
    discrete_step = jax.nn.softplus(step_raw + step_size_bias[None, :])
    step_logarithm = discrete_step * (-jnp.exp(log_decay_rate))[None, :] + decay_spikes.T
    blocks = SEQUENCE_TOKENS // BLOCK
    per_group = MIXER_HEADS // GROUPS
    input_blocks = seq_input.reshape(blocks, BLOCK, MIXER_HEADS, HEAD_DIM)
    weighted = input_blocks * discrete_step.reshape(blocks, BLOCK, MIXER_HEADS, 1)
    write_blocks = seq_write.reshape(blocks, BLOCK, GROUPS, STATE)
    read_blocks = seq_read.reshape(blocks, BLOCK, GROUPS, STATE)
    cumulative = jnp.cumsum(step_logarithm.reshape(blocks, BLOCK, MIXER_HEADS), axis=1)
    causal = lax.broadcasted_iota(jnp.int32, (BLOCK, BLOCK), 0) >= lax.broadcasted_iota(jnp.int32, (BLOCK, BLOCK), 1)

    def one_block(carried_state, inputs):
        block_weighted, block_write, block_read, block_cum = inputs
        write_heads = jnp.repeat(block_write, per_group, axis=1)
        read_heads = jnp.repeat(block_read, per_group, axis=1)
        scores = jnp.einsum('lhm,shm->lsh', read_heads, write_heads, precision=highest)
        damping = jnp.exp(jnp.where(causal[:, :, None], block_cum[:, None, :] - block_cum[None, :, :], -jnp.inf))
        within = jnp.einsum('lsh,shp->lhp', scores * damping, block_weighted, precision=highest)
        from_before = jnp.einsum('lhm,hpm->lhp', read_heads, carried_state, precision=highest) * jnp.exp(block_cum)[:, :, None]
        to_end = jnp.exp(block_cum[-1:, :] - block_cum)
        new_state = jnp.einsum('shm,shp->hpm', write_heads * to_end[:, :, None], block_weighted, precision=highest)
        return (carried_state * jnp.exp(block_cum[-1])[:, None, None] + new_state, within + from_before)
    _, block_outputs = lax.scan(one_block, jnp.zeros((MIXER_HEADS, HEAD_DIM, STATE), jnp.float32), (weighted, write_blocks, read_blocks, cumulative))
    head_out = block_outputs + direct_path_weight[None, None, :, None] * input_blocks
    head_out = head_out.reshape(SEQUENCE_TOKENS, MIXER_HEADS * HEAD_DIM)
    gated_heads = (head_out * jax.nn.silu(out_gate.astype(jnp.float32))).reshape(SEQUENCE_TOKENS, MIXER_HEADS, HEAD_DIM)
    normalized = gated_heads * lax.rsqrt(lax.optimization_barrier(jnp.mean(gated_heads * gated_heads, axis=2, keepdims=True)) + epsilon)
    state_part = (normalized.reshape(SEQUENCE_TOKENS, MIXER_HEADS * HEAD_DIM) * head_norm_scale.astype(jnp.float32)).astype(jnp.bfloat16)
    share_conv = CONV // N_TP
    share_state = MIXER_HEADS * HEAD_DIM // N_TP
    running = jnp.zeros((SEQUENCE_TOKENS, D), jnp.float32)
    for head_block in range(N_TP):
        conv_slice = slice(head_block * share_conv, (head_block + 1) * share_conv)
        state_slice = slice(head_block * share_state, (head_block + 1) * share_state)
        partial_sum = jnp.dot(mixer_part[:, conv_slice], conv_output_weight[conv_slice], preferred_element_type=jnp.float32)
        partial_sum = partial_sum + jnp.dot(state_part[:, state_slice], state_output_weight[state_slice], preferred_element_type=jnp.float32)
        rounded = lax.optimization_barrier(partial_sum.astype(jnp.bfloat16))
        running = running + rounded.astype(jnp.float32)
    return running.astype(jnp.bfloat16)
```

```python
import functools

import jax
import jax.numpy as jnp
from jax import lax
from jax.experimental import pallas as pl
from jax.experimental.pallas import tpu as pltpu
from jax.sharding import PartitionSpec as P

HEAD_DIM = 64
STATE = 128
PLAIN_BLOCK = 64
CHUNK = 128
HALO = 16
QIN = 2
CORES = 2
epsilon = 1e-05
highest = lax.Precision.HIGHEST
f32 = jnp.float32
bf16 = jnp.bfloat16
MESH = pl.DeviceIdType.MESH


def nt(a, b, precision=None):
    return lax.dot_general(
        a, b, (((1,), (1,)), ((), ())), preferred_element_type=f32, precision=precision
    )


def silu(v):
    return v / (1.0 + jnp.exp(-v))


def kernel(
    n,
    T,
    tokens,
    in_scale,
    w_outer,
    w_inner,
    w_value,
    w_ogate,
    w_state,
    w_write,
    w_read,
    step_w,
    taps_conv,
    taps_in,
    taps_wr,
    taps_rd,
    bias,
    rate,
    spikes,
    direct,
    hscale,
    o_conv,
    o_state,
    out,
    wbuf,
    obuf,
    norm,
    acc,
    mixbuf,
    xbuf,
    wrbuf,
    rdbuf,
    ybuf,
    cumbuf,
    stbuf,
    st_send,
    st_recv,
    apart,
    part,
    r1,
    p2,
    r2,
    loc_sem,
    ws_sem,
    wr_sem,
    os_sem,
    or_sem,
    ts_sem,
    tr_sem,
    h_sem,
    ss_sem,
    sr_sem,
    r1s_sem,
    r1r_sem,
    r2s_sem,
    r2r_sem,
):
    sp = lax.axis_index("sp")
    tp = lax.axis_index("tp")
    rows, width = tokens.shape
    kdim = w_outer.shape[0]
    cdim = w_outer.shape[1]
    half = wbuf.shape[3]
    length = rows * T
    heads_width = xbuf.shape[1]
    heads = heads_width // HEAD_DIM
    n_half = n // 2

    barrier = pltpu.get_barrier_semaphore()
    for d in range(1, n):
        pl.semaphore_signal(
            barrier, inc=1, device_id={"sp": lax.rem(sp + d, n)}, device_id_type=MESH
        )
    for d in range(1, T):
        pl.semaphore_signal(
            barrier, inc=1, device_id={"tp": lax.rem(tp + d, T)}, device_id_type=MESH
        )

    locals_ = []
    at = 0
    for ref in (w_outer, w_inner, w_value):
        locals_.append((ref, wbuf.at[0, 0, :, at : at + ref.shape[1]]))
        at += ref.shape[1]
    at = 0
    for ref in (w_ogate, w_state, w_write, w_read):
        locals_.append((ref, wbuf.at[0, 1, :, at : at + ref.shape[1]]))
        at += ref.shape[1]
    locals_.append((o_conv, obuf.at[0, 0]))
    locals_.append((o_state, obuf.at[0, 1]))
    local_copies = [
        pltpu.make_async_copy(src, dst, loc_sem.at[i]) for i, (src, dst) in enumerate(locals_)
    ]
    for copy in local_copies:
        copy.start()

    def pos_of(index):
        odd = lax.rem(index, 2)
        low = lax.div(index, 2)
        return (1 - odd) * low + odd * (n - 1 - low)

    def index_of(pos):
        high = lax.div(pos, n_half)
        return (1 - high) * 2 * pos + high * (2 * (n - 1 - pos) + 1)

    pos = pos_of(sp)
    right = index_of(lax.rem(pos + 1, n))
    left = index_of(lax.rem(pos + n - 1, n))
    neighbour = (right, left)

    def owner_of(s, way):
        return index_of(lax.rem(pos + n - s, n) if way == 0 else lax.rem(pos + s, n))

    piece = kdim // QIN

    def w_copy(s, q, way):
        return pltpu.make_async_remote_copy(
            src_ref=wbuf.at[s, way, pl.ds(q * piece, piece)],
            dst_ref=wbuf.at[s + 1, way, pl.ds(q * piece, piece)],
            send_sem=ws_sem.at[s, q, way],
            recv_sem=wr_sem.at[s, q, way],
            device_id={"sp": neighbour[way]},
            device_id_type=MESH,
        )

    def o_copy(s, way):
        return pltpu.make_async_remote_copy(
            src_ref=obuf.at[s, way],
            dst_ref=obuf.at[s + 1, way],
            send_sem=os_sem.at[s, way],
            recv_sem=or_sem.at[s, way],
            device_id={"sp": neighbour[way]},
            device_id_type=MESH,
        )

    def forward(s):
        for q in range(QIN):
            for way in range(2):

                @pl.when(s > 0)
                def _():
                    w_copy(s - 1, q, way).wait_recv()

                @pl.when(s < n - 1)
                def _():
                    w_copy(s, q, way).start()

    def o_forward(s):
        for way in range(2):

            @pl.when(s > 0)
            def _():
                o_copy(s - 1, way).wait_recv()

            @pl.when(s < n - 1)
            def _():
                o_copy(s, way).start()

    own_at = pl.multiple_of(HALO + tp * rows, HALO)
    x = tokens[...].astype(f32)
    x = x * lax.rsqrt(jnp.mean(x * x, axis=1, keepdims=True) + epsilon)
    norm[pl.ds(own_at, rows), :] = (x * in_scale[...].astype(f32)).astype(bf16)
    acc[...] = jnp.zeros_like(acc)

    for copy in local_copies:
        copy.wait()
    pl.semaphore_wait(barrier, n - 1 + T - 1)

    forward(0)

    def t_copy(d):
        return pltpu.make_async_remote_copy(
            src_ref=norm.at[pl.ds(own_at, rows)],
            dst_ref=norm.at[pl.ds(own_at, rows)],
            send_sem=ts_sem.at[d],
            recv_sem=tr_sem.at[d],
            device_id={"tp": lax.rem(tp + d, T)},
            device_id_type=MESH,
        )

    for d in range(1, T):
        t_copy(d).start()

    mid = n_half - 1

    def ahead(s, carry):
        forward(s)
        return carry

    lax.fori_loop(1, max(mid, 1), ahead, 0)

    def t_wait(d):
        source = pl.multiple_of(HALO + lax.rem(tp + T - d, T) * rows, HALO)
        pltpu.make_async_remote_copy(
            src_ref=norm.at[pl.ds(source, rows)],
            dst_ref=norm.at[pl.ds(source, rows)],
            send_sem=ts_sem.at[d],
            recv_sem=tr_sem.at[d],
            device_id={"tp": lax.rem(tp + d, T)},
            device_id_type=MESH,
        ).wait_recv()

    for d in range(1, T):
        t_wait(d)

    def h_copy():
        return pltpu.make_async_remote_copy(
            src_ref=norm.at[pl.ds(length, HALO)],
            dst_ref=norm.at[pl.ds(0, HALO)],
            send_sem=h_sem.at[0],
            recv_sem=h_sem.at[1],
            device_id={"sp": lax.rem(sp + 1, n)},
            device_id_type=MESH,
        )

    @pl.when(sp < n - 1)
    def _():
        h_copy().start()

    forward(max(mid, 1))

    @pl.when(sp > 0)
    def _():
        h_copy().wait_recv()

    @pl.when(sp == 0)
    def _():
        norm[0:HALO, :] = jnp.zeros((HALO, width), bf16)

    def project(s):
        for way in range(2):
            at = pl.multiple_of(owner_of(s, way) * kdim, kdim)
            lhs = norm[:, pl.ds(at, kdim)]
            for c in range(0, half, 256):
                acc[:, way * half + c : way * half + c + 256] += jnp.dot(
                    lhs, wbuf[s, way, :, c : c + 256], preferred_element_type=f32
                )

    start = max(mid, 1)

    def body(s, carry):
        @pl.when(s > start)
        def _():
            forward(s)

        project(s)

        @pl.when(s - start < start)
        def _():
            project(s - start)

        return carry

    lax.fori_loop(start, n, body, 0)

    o_forward(0)
    o_done = [1]
    stages = 2 * (length // CHUNK)
    per_stage = -(-(n - 1) // max(stages - 1, 1))

    def relay(k=per_stage):
        lo = o_done[0]
        hi = min(lo + k, n)
        o_done[0] = hi
        for s in range(lo, hi) if hi - lo <= 4 else ():
            o_forward(s)
        if hi - lo > 4:

            def go(s, carry):
                o_forward(s)
                return carry

            lax.fori_loop(lo, hi, go, 0)

    step = jax.nn.softplus(nt(step_w[...], norm[HALO:, :])[0:8] + bias[...])
    logs = -step * jnp.exp(rate[...]) + spikes[...]
    r_id = lax.broadcasted_iota(jnp.int32, (CHUNK, CHUNK), 0)
    c_id = lax.broadcasted_iota(jnp.int32, (CHUNK, CHUNK), 1)
    causal = r_id >= c_id
    lower = causal.astype(f32)
    eye = (r_id == c_id).astype(f32)
    lane = lax.broadcasted_iota(jnp.int32, (1, heads_width), 1)

    def spread(columns):
        full = jnp.broadcast_to(columns[:, 0:1], (columns.shape[0], heads_width))
        for h in range(1, heads):
            full = jnp.where(lane >= h * HEAD_DIM, columns[:, h : h + 1], full)
        return full

    def taps(u, weights):
        k_taps = weights.shape[0]
        w = weights[...].astype(f32)
        total = w[k_taps - 1 : k_taps] * u[8:]
        for k in range(k_taps - 1):
            total = total + w[k : k + 1] * pltpu.roll(u, k_taps - 1 - k, 0)[8:]
        return total

    blocks = length // CHUNK
    running = jnp.zeros((STATE, heads_width), f32)
    before = jnp.zeros((1, heads_width), f32)
    at_outer, at_inner, at_value, at_ogate, at_state = (i * cdim for i in range(5))
    at_write = 5 * cdim
    at_read = at_write + STATE
    for b in range(blocks):
        t0 = b * CHUNK
        take = slice(t0 + HALO - 8, t0 + HALO + CHUNK)
        own = slice(t0 + HALO, t0 + HALO + CHUNK)

        def field(begin, size, span):
            return acc[span, begin : begin + size].astype(bf16).astype(f32)

        product = field(at_inner, cdim, take) * field(at_value, cdim, take)
        mix = field(at_outer, cdim, own) * taps(product, taps_conv)
        apart[t0 : t0 + CHUNK, 0:cdim] = mix.astype(bf16)
        xs = silu(taps(field(at_state, cdim, take), taps_in))
        wr = silu(taps(field(at_write, STATE, take), taps_wr))
        rd = silu(taps(field(at_read, STATE, take), taps_rd))
        span = slice(t0, t0 + CHUNK)
        cum = nt(lower, logs[:, span], highest)
        steps = nt(eye, step[:, span], highest)
        cum_wide = spread(cum)
        weighted = xs * spread(steps)
        xbuf[span, :] = xs
        mixbuf[span, :] = weighted.astype(bf16)
        wrbuf[span, :] = wr.astype(bf16)
        rdbuf[span, :] = rd.astype(bf16)
        cumbuf[span, :] = cum_wide
        last = cum_wide[CHUNK - 1 : CHUNK]
        scaled = (weighted * jnp.exp(last - cum_wide)).astype(bf16)
        stbuf[b] = running
        running = running * jnp.exp(last) + jnp.dot(
            wr.T.astype(bf16), scaled, preferred_element_type=f32
        )
        before = before + last
        relay()
    st_send[0:STATE, :] = running.astype(bf16)
    st_send[STATE:, :] = jnp.broadcast_to(jnp.exp(before), (HALO, heads_width)).astype(bf16)

    def s_copy(k, slot):
        return pltpu.make_async_remote_copy(
            src_ref=st_send,
            dst_ref=st_recv.at[slot],
            send_sem=ss_sem.at[k],
            recv_sem=sr_sem.at[slot],
            device_id={"sp": k},
            device_id_type=MESH,
        )

    def within(b):
        t0 = b * CHUNK
        span = slice(t0, t0 + CHUNK)
        scores = nt(rdbuf[span, :], wrbuf[span, :])
        cum_t = lax.dot_general(
            logs[:, span], lower, (((1,), (1,)), ((), ())),
            preferred_element_type=f32, precision=highest,
        )
        for pair in range(0, heads_width, 128):
            both = []
            for h in range(pair // HEAD_DIM, (pair + 128) // HEAD_DIM):
                diff = cumbuf[span, h * HEAD_DIM : h * HEAD_DIM + 1] - cum_t[h : h + 1, :]
                damped = scores * jnp.exp(jnp.where(causal, diff, -1e30))
                both.append(
                    jnp.dot(
                        damped.astype(bf16), mixbuf[span, pair : pair + 128],
                        preferred_element_type=f32,
                    )
                )
            first = lax.broadcasted_iota(jnp.int32, (1, 128), 1) < HEAD_DIM
            ybuf[span, pair : pair + 128] = jnp.where(first, both[0], both[1])

    def s_start(k, carry):
        s_copy(k, sp).start()
        return carry

    lax.fori_loop(sp + 1, n, s_start, 0)
    for b in range(blocks):
        within(b)
        relay()
    relay(n)

    def s_take(k, arriving):
        s_copy(k, k).wait_recv()
        got = st_recv[k].astype(f32)
        return arriving * got[STATE : STATE + 1] + got[0:STATE]

    arriving = lax.fori_loop(0, sp, s_take, jnp.zeros((STATE, heads_width), f32))

    group = (
        lax.div(lax.broadcasted_iota(jnp.int32, (heads_width, heads_width), 0), HEAD_DIM)
        == lax.div(lax.broadcasted_iota(jnp.int32, (heads_width, heads_width), 1), HEAD_DIM)
    ).astype(bf16)
    before = jnp.zeros((1, heads_width), f32)
    for b in range(blocks):
        t0 = b * CHUNK
        span = slice(t0, t0 + CHUNK)
        own = slice(t0 + HALO, t0 + HALO + CHUNK)
        cum_wide = cumbuf[span, :]
        entering = (stbuf[b] + jnp.exp(before) * arriving).astype(bf16)
        before = before + cum_wide[CHUNK - 1 : CHUNK]
        head_out = (
            ybuf[span, :]
            + jnp.dot(rdbuf[span, :], entering, preferred_element_type=f32) * jnp.exp(cum_wide)
            + direct[...] * xbuf[span, :]
        )
        og = acc[own, at_ogate : at_ogate + cdim].astype(bf16).astype(f32)
        gated = head_out * silu(og)
        square = jnp.dot((gated * gated).astype(bf16), group, preferred_element_type=f32)
        normalized = gated * lax.rsqrt(square * (1.0 / HEAD_DIM) + epsilon)
        apart[span, cdim:] = (normalized * hscale[...].astype(f32)).astype(bf16)

    ocols = o_conv.shape[1]

    def project_out(k, carry):
        kp = pos_of(k)
        a = lax.rem(pos + n - kp, n)
        c = lax.rem(kp + n - pos, n)
        cols = pl.ds(pl.multiple_of(k * ocols, ocols), ocols)
        part[:, cols] = (
            jnp.dot(apart[:, 0:cdim], obuf[a, 0], preferred_element_type=f32)
            + jnp.dot(apart[:, cdim:], obuf[c, 1], preferred_element_type=f32)
        ).astype(bf16)
        return carry

    Y = T // CORES
    core = lax.rem(tp, CORES)
    chip = lax.div(tp, CORES)
    partner = chip * CORES + 1 - core
    pieces = r1.shape[1]
    pcols = width // pieces

    def block_rows(y, c):
        return pl.ds(pl.multiple_of((y * CORES + c) * rows, rows), rows)

    def r1_copy(d, c):
        y = lax.rem(chip + d, Y)
        return pltpu.make_async_remote_copy(
            src_ref=part.at[block_rows(y, 1 - core), pl.ds(c * pcols, pcols)],
            dst_ref=r1.at[d, c],
            send_sem=r1s_sem.at[d, c],
            recv_sem=r1r_sem.at[d, c],
            device_id={"tp": partner},
            device_id_type=MESH,
        )

    def r2_copy(d, c):
        return pltpu.make_async_remote_copy(
            src_ref=p2.at[d, c],
            dst_ref=r2.at[d, c],
            send_sem=r2s_sem.at[d, c],
            recv_sem=r2r_sem.at[d, c],
            device_id={"tp": lax.rem(chip + d, Y) * CORES + core},
            device_id_type=MESH,
        )

    per_piece = n // pieces
    for c in range(pieces):
        lax.fori_loop(c * per_piece, (c + 1) * per_piece, project_out, 0)
        for d in range(1, Y):
            r1_copy(d, c).start()
        r1_copy(0, c).start()
        if c > 0:
            for d in range(1, Y):
                reduce_far(d, c - 1, r1_copy, r2_copy, part, r1, p2, block_rows, chip, Y, core, pcols)
    for d in range(1, Y):
        reduce_far(d, pieces - 1, r1_copy, r2_copy, part, r1, p2, block_rows, chip, Y, core, pcols)
    for c in range(pieces):
        r1_copy(0, c).wait_recv()
        cols = slice(c * pcols, (c + 1) * pcols)
        total = part[block_rows(chip, core), cols].astype(f32) + r1[0, c].astype(f32)
        for d in range(1, Y):
            r2_copy(d, c).wait_recv()
            total = total + r2[d, c].astype(f32)
        out[:, cols] = total.astype(bf16)

    def w_drain(s, carry):
        for way in range(2):
            for q in range(QIN):
                w_copy(s, q, way).wait_send()
            o_copy(s, way).wait_send()
        return carry

    lax.fori_loop(0, n - 1, w_drain, 0)
    for d in range(1, T):
        t_copy(d).wait_send()

    @pl.when(sp < n - 1)
    def _():
        h_copy().wait_send()

    def s_drain(k, carry):
        s_copy(k, sp).wait_send()
        return carry

    lax.fori_loop(sp + 1, n, s_drain, 0)
    for c in range(pieces):
        for d in range(Y):
            r1_copy(d, c).wait_send()
        for d in range(1, Y):
            r2_copy(d, c).wait_send()


def reduce_far(d, c, r1_copy, r2_copy, part, r1, p2, block_rows, chip, Y, core, pcols):
    r1_copy(d, c).wait_recv()
    y = lax.rem(chip + d, Y)
    p2[d, c] = (
        part[block_rows(y, core), c * pcols : (c + 1) * pcols].astype(f32) + r1[d, c].astype(f32)
    ).astype(bf16)
    r2_copy(d, c).start()


def shifted(shard, axis, by):
    devices = lax.axis_size(axis)
    pairs = [(i, i + by) for i in range(devices) if 0 <= i + by < devices]
    return lax.ppermute(shard, axis, pairs)


def prefix(shard, axis, combine, identity):
    devices, index = (lax.axis_size(axis), lax.axis_index(axis))
    everything = jax.tree.map(
        lambda part, kind: lax.all_gather(part.astype(kind), axis),
        shard,
        (jnp.bfloat16, jnp.bfloat16),
    )
    start = jax.tree.map(
        lambda part, zero: jnp.broadcast_to(jnp.asarray(zero, part.dtype), part.shape),
        shard,
        identity,
    )

    def turn(k, before):
        reached = k < index
        new = combine(
            before, jax.tree.map(lambda part, own: part[k].astype(own.dtype), everything, shard)
        )
        return jax.tree.map(lambda a, b: jnp.where(reached, a, b), new, before)

    return lax.fori_loop(0, devices, turn, start)


def causal_taps(values, rim_rows, tap_weights):
    tap_count = tap_weights.shape[0]
    length = values.shape[0]
    padded = jnp.concatenate([rim_rows, values], axis=0)
    running = tap_weights[0] * padded[0:length]
    for offset in range(1, tap_count):
        running = running + tap_weights[offset] * padded[offset : offset + length]
    return running


def combine_states(earlier, later):
    return (earlier[0] * later[0], earlier[1] * later[0][:, None, None] + later[1])


def plain_path(
    tokens,
    input_norm_scale,
    outer_gate_weight,
    inner_gate_weight,
    value_weight_matrix,
    output_gate_weight,
    state_input_weight,
    write_key_weight,
    read_key_weight,
    step_size_weight,
    gated_conv_weight,
    input_conv_weight,
    write_conv_weight,
    read_conv_weight,
    step_size_bias,
    log_decay_rate,
    decay_spikes,
    direct_path_weight,
    head_norm_scale,
    conv_output_weight,
    state_output_weight,
):
    token_rows = tokens.astype(jnp.float32)
    scaled = token_rows * lax.rsqrt(
        jnp.mean(token_rows * token_rows, axis=1, keepdims=True) + epsilon
    )
    normed_own = (scaled * input_norm_scale.astype(jnp.float32)).astype(jnp.bfloat16)
    normed = lax.all_gather(normed_own, "tp", axis=0, tiled=True)
    length = normed.shape[0]
    pieces = (
        lax.all_gather(outer_gate_weight, "sp", axis=0, tiled=True),
        lax.all_gather(inner_gate_weight, "sp", axis=0, tiled=True),
        lax.all_gather(value_weight_matrix, "sp", axis=0, tiled=True),
        lax.all_gather(output_gate_weight, "sp", axis=0, tiled=True),
        lax.all_gather(state_input_weight, "sp", axis=0, tiled=True),
        lax.all_gather(write_key_weight, "sp", axis=0, tiled=True),
        lax.all_gather(read_key_weight, "sp", axis=0, tiled=True),
    )
    projected = tuple(
        (jnp.dot(normed, weight_rows, preferred_element_type=jnp.float32) for weight_rows in pieces)
    )
    outer_gate, inner_gate, conv_input, out_gate, state_input, write_keys, read_keys = [
        member.astype(jnp.bfloat16) for member in projected
    ]
    step_raw = jnp.dot(normed, step_size_weight, preferred_element_type=jnp.float32)
    short_rim = gated_conv_weight.shape[0] - 1
    state_rim = input_conv_weight.shape[0] - 1
    rim_rows = shifted(
        (
            inner_gate[length - short_rim :],
            conv_input[length - short_rim :],
            state_input[length - state_rim :],
            write_keys[length - state_rim :],
            read_keys[length - state_rim :],
        ),
        "sp",
        1,
    )
    product = inner_gate.astype(jnp.float32) * conv_input.astype(jnp.float32)
    rim_product = rim_rows[0].astype(jnp.float32) * rim_rows[1].astype(jnp.float32)
    mixer_part = (
        outer_gate.astype(jnp.float32)
        * causal_taps(product, rim_product, gated_conv_weight.astype(jnp.float32))
    ).astype(jnp.bfloat16)
    seq_input = jax.nn.silu(
        causal_taps(
            state_input.astype(jnp.float32),
            rim_rows[2].astype(jnp.float32),
            input_conv_weight.astype(jnp.float32),
        )
    )
    seq_write = jax.nn.silu(
        causal_taps(
            write_keys.astype(jnp.float32),
            rim_rows[3].astype(jnp.float32),
            write_conv_weight.astype(jnp.float32),
        )
    )
    seq_read = jax.nn.silu(
        causal_taps(
            read_keys.astype(jnp.float32),
            rim_rows[4].astype(jnp.float32),
            read_conv_weight.astype(jnp.float32),
        )
    )
    discrete_step = jax.nn.softplus(step_raw + step_size_bias[None, :])
    step_logarithm = discrete_step * (-jnp.exp(log_decay_rate))[None, :] + decay_spikes.T
    heads_here = discrete_step.shape[1]
    groups_here = seq_write.shape[1] // STATE
    per_group = heads_here // groups_here
    blocks = length // PLAIN_BLOCK
    input_blocks = seq_input.reshape(blocks, PLAIN_BLOCK, heads_here, HEAD_DIM)
    weighted = input_blocks * discrete_step.reshape(blocks, PLAIN_BLOCK, heads_here, 1)
    write_blocks = jnp.repeat(
        seq_write.reshape(blocks, PLAIN_BLOCK, groups_here, STATE), per_group, axis=2
    )
    read_blocks = jnp.repeat(seq_read.reshape(blocks, PLAIN_BLOCK, groups_here, STATE), per_group, axis=2)
    cumulative = jnp.cumsum(step_logarithm.reshape(blocks, PLAIN_BLOCK, heads_here), axis=1)
    causal = lax.broadcasted_iota(jnp.int32, (PLAIN_BLOCK, PLAIN_BLOCK), 0) >= lax.broadcasted_iota(
        jnp.int32, (PLAIN_BLOCK, PLAIN_BLOCK), 1
    )
    scores = jnp.einsum("clhm,cshm->clsh", read_blocks, write_blocks, precision=highest)
    damping = jnp.exp(
        jnp.where(
            causal[None, :, :, None],
            cumulative[:, :, None, :] - cumulative[:, None, :, :],
            -jnp.inf,
        )
    )
    within_block = jnp.einsum("clsh,cshp->clhp", scores * damping, weighted, precision=highest)
    to_end = jnp.exp(cumulative[:, -1:, :] - cumulative)
    block_states = jnp.einsum(
        "cshm,cshp->chpm", write_blocks * to_end[..., None], weighted, precision=highest
    )
    block_logs = cumulative[:, -1, :]

    def advance(carried_state, inputs):
        contribution, block_log = inputs
        return (carried_state * jnp.exp(block_log)[:, None, None] + contribution, carried_state)

    own_total, own_before = lax.scan(
        advance, jnp.zeros(block_states.shape[1:], jnp.float32), (block_states, block_logs)
    )
    total_log = jnp.sum(block_logs, axis=0)
    arriving = prefix(
        (jnp.exp(total_log), own_total),
        "sp",
        combine_states,
        (jnp.ones_like(total_log), jnp.zeros_like(own_total)),
    )[1]
    before_logs = jnp.cumsum(block_logs, axis=0) - block_logs
    entering = own_before + jnp.exp(before_logs)[:, :, None, None] * arriving[None]
    from_before = (
        jnp.einsum("clhm,chpm->clhp", read_blocks, entering, precision=highest)
        * jnp.exp(cumulative)[..., None]
    )
    head_out = within_block + from_before + direct_path_weight[None, None, :, None] * input_blocks
    head_out = head_out.reshape(length, heads_here * HEAD_DIM)
    gated_heads = (head_out * jax.nn.silu(out_gate.astype(jnp.float32))).reshape(
        length, heads_here, HEAD_DIM
    )
    normalized = gated_heads * lax.rsqrt(
        jnp.mean(gated_heads * gated_heads, axis=2, keepdims=True) + epsilon
    )
    state_part = (
        normalized.reshape(length, heads_here * HEAD_DIM) * head_norm_scale.astype(jnp.float32)
    ).astype(jnp.bfloat16)
    wide_mixer, wide_state = (
        lax.all_gather(conv_output_weight, "sp", axis=1, tiled=True),
        lax.all_gather(state_output_weight, "sp", axis=1, tiled=True),
    )
    return lax.psum_scatter(
        (
            jnp.dot(mixer_part, wide_mixer, preferred_element_type=jnp.float32)
            + jnp.dot(state_part, wide_state, preferred_element_type=jnp.float32)
        ).astype(jnp.bfloat16),
        "tp",
        scatter_dimension=0,
        tiled=True,
    )


def per_device(
    tokens, input_norm_scale, outer_gate_weight, inner_gate_weight, value_weight_matrix,
    output_gate_weight, state_input_weight, write_key_weight, read_key_weight, step_size_weight,
    gated_conv_weight, input_conv_weight, write_conv_weight, read_conv_weight, step_size_bias,
    log_decay_rate, decay_spikes, direct_path_weight, head_norm_scale, conv_output_weight,
    state_output_weight,
):
    n, T = lax.axis_size("sp"), lax.axis_size("tp")
    rows, width = tokens.shape
    kdim, cdim = outer_gate_weight.shape
    heads = step_size_bias.shape[0]
    hw = heads * HEAD_DIM
    half = 3 * cdim
    length = rows * T
    ocols = conv_output_weight.shape[1]
    if kdim % 128 or ocols % 128 or n % 2 or T % CORES or write_key_weight.shape[1] != STATE:
        return plain_path(
            tokens, input_norm_scale, outer_gate_weight, inner_gate_weight,
            value_weight_matrix, output_gate_weight, state_input_weight, write_key_weight,
            read_key_weight, step_size_weight, gated_conv_weight, input_conv_weight,
            write_conv_weight, read_conv_weight, step_size_bias, log_decay_rate, decay_spikes,
            direct_path_weight, head_norm_scale, conv_output_weight, state_output_weight,
        )
    Y = T // CORES
    pieces = 4 if n % 4 == 0 else 1
    pad = 8 - heads
    step_w = jnp.pad(step_size_weight.T, ((0, 16 - heads), (0, 0)))
    bias = jnp.pad(step_size_bias, (0, pad))[:, None]
    rate = jnp.pad(log_decay_rate, (0, pad))[:, None]
    spikes = jnp.pad(decay_spikes, ((0, pad), (0, 0)))
    direct = jnp.repeat(direct_path_weight, HEAD_DIM)[None, :]
    vm = pl.BlockSpec(memory_space=pltpu.VMEM)
    hbm = pl.BlockSpec(memory_space=pl.ANY)
    dma = pltpu.SemaphoreType.DMA
    return pl.pallas_call(
        functools.partial(kernel, n, T),
        out_shape=jax.ShapeDtypeStruct((rows, width), bf16),
        in_specs=[vm] * 2 + [hbm] * 7 + [vm] * 10 + [hbm] * 2,
        out_specs=vm,
        scratch_shapes=[
            pltpu.VMEM((n, 2, kdim, half), bf16),
            pltpu.VMEM((n, 2, cdim, ocols), bf16),
            pltpu.VMEM((HALO + length, width), bf16),
            pltpu.VMEM((HALO + length, 2 * half), f32),
            pltpu.VMEM((length, hw), bf16),
            pltpu.VMEM((length, hw), f32),
            pltpu.VMEM((length, STATE), bf16),
            pltpu.VMEM((length, STATE), bf16),
            pltpu.VMEM((length, hw), f32),
            pltpu.VMEM((length, hw), f32),
            pltpu.VMEM((length // CHUNK, STATE, hw), f32),
            pltpu.VMEM((STATE + HALO, hw), bf16),
            pltpu.VMEM((n, STATE + HALO, hw), bf16),
            pltpu.VMEM((length, cdim + hw), bf16),
            pltpu.VMEM((length, width), bf16),
            pltpu.VMEM((Y, pieces, rows, width // pieces), bf16),
            pltpu.VMEM((Y, pieces, rows, width // pieces), bf16),
            pltpu.VMEM((Y, pieces, rows, width // pieces), bf16),
            dma((9,)),
            dma((n, QIN, 2)),
            dma((n, QIN, 2)),
            dma((n, 2)),
            dma((n, 2)),
            dma((T,)),
            dma((T,)),
            dma((2,)),
            dma((n,)),
            dma((n,)),
            dma((Y, pieces)),
            dma((Y, pieces)),
            dma((Y, pieces)),
            dma((Y, pieces)),
        ],
        compiler_params=pltpu.CompilerParams(
            collective_id=0, has_side_effects=True, vmem_limit_bytes=62 * 1024 * 1024
        ),
    )(
        tokens, input_norm_scale[None, :], outer_gate_weight, inner_gate_weight,
        value_weight_matrix, output_gate_weight, state_input_weight, write_key_weight,
        read_key_weight, step_w, gated_conv_weight, input_conv_weight, write_conv_weight,
        read_conv_weight, bias, rate, spikes, direct, head_norm_scale[None, :],
        conv_output_weight, state_output_weight,
    )


def solution(mesh):
    placed = (
        (P(("sp", "tp"), None), P())
        + (P("sp", "tp"),) * 7
        + (P(None, "tp"),) * 5
        + (P("tp"), P("tp"), P("tp", "sp"), P("tp"), P("tp"), P("tp", "sp"), P("tp", "sp"))
    )
    return jax.shard_map(
        per_device, mesh=mesh, in_specs=placed, out_specs=P(("sp", "tp"), None), check_vma=False
    )
```

```python
import functools

import jax
import jax.numpy as jnp
from jax import lax
from jax.experimental import pallas as pl
from jax.experimental.pallas import tpu as pltpu
from jax.sharding import PartitionSpec as P

HEAD_DIM = 64
STATE = 128
PLAIN_BLOCK = 64
CHUNK = 128
HALO = 16
QIN = 2
QOUT = 2
CORES = 2
epsilon = 1e-05
highest = lax.Precision.HIGHEST
f32 = jnp.float32
bf16 = jnp.bfloat16
MESH = pl.DeviceIdType.MESH


def nt(a, b, precision=None):
    return lax.dot_general(
        a, b, (((1,), (1,)), ((), ())), preferred_element_type=f32, precision=precision
    )


def silu(v):
    return v / (1.0 + jnp.exp(-v))


def kernel(
    n,
    T,
    tokens,
    in_scale,
    w_outer,
    w_inner,
    w_value,
    w_ogate,
    w_state,
    w_write,
    w_read,
    step_w,
    taps_conv,
    taps_in,
    taps_wr,
    taps_rd,
    bias,
    rate,
    spikes,
    direct,
    hscale,
    o_conv,
    o_state,
    out,
    wbuf,
    obuf,
    norm,
    acc,
    mixbuf,
    xbuf,
    wrbuf,
    rdbuf,
    ybuf,
    cumbuf,
    stbuf,
    st_send,
    st_recv,
    e_send,
    e_recv,
    pair_buf,
    apart,
    part,
    r1,
    p2,
    r2,
    loc_sem,
    ws_sem,
    wr_sem,
    os_sem,
    or_sem,
    ts_sem,
    tr_sem,
    h_sem,
    x_sem,
    e_sem,
    r1s_sem,
    r1r_sem,
    r2s_sem,
    r2r_sem,
):
    sp = lax.axis_index("sp")
    tp = lax.axis_index("tp")
    rows, width = tokens.shape
    kdim = w_outer.shape[0]
    cdim = w_outer.shape[1]
    half = wbuf.shape[3]
    length = rows * T
    heads_width = xbuf.shape[1]
    heads = heads_width // HEAD_DIM
    n_half = n // 2

    barrier = pltpu.get_barrier_semaphore()
    for d in range(1, n):
        pl.semaphore_signal(
            barrier, inc=1, device_id={"sp": lax.rem(sp + d, n)}, device_id_type=MESH
        )
    for d in range(1, T):
        pl.semaphore_signal(
            barrier, inc=1, device_id={"tp": lax.rem(tp + d, T)}, device_id_type=MESH
        )

    locals_ = []
    at = 0
    for ref in (w_outer, w_inner, w_value):
        locals_.append((ref, wbuf.at[0, 0, :, at : at + ref.shape[1]]))
        at += ref.shape[1]
    at = 0
    for ref in (w_ogate, w_state, w_write, w_read):
        locals_.append((ref, wbuf.at[0, 1, :, at : at + ref.shape[1]]))
        at += ref.shape[1]
    ohalf = obuf.shape[3]
    for way in range(2):
        cut = pl.ds(way * ohalf, ohalf)
        locals_.append((o_conv.at[:, cut], obuf.at[0, way, pl.ds(0, cdim)]))
        locals_.append((o_state.at[:, cut], obuf.at[0, way, pl.ds(cdim, heads_width)]))
    local_copies = [
        pltpu.make_async_copy(src, dst, loc_sem.at[i]) for i, (src, dst) in enumerate(locals_)
    ]
    for copy in local_copies:
        copy.start()

    def pos_of(index):
        odd = lax.rem(index, 2)
        low = lax.div(index, 2)
        return (1 - odd) * low + odd * (n - 1 - low)

    def index_of(pos):
        high = lax.div(pos, n_half)
        return (1 - high) * 2 * pos + high * (2 * (n - 1 - pos) + 1)

    pos = pos_of(sp)
    right = index_of(lax.rem(pos + 1, n))
    left = index_of(lax.rem(pos + n - 1, n))
    neighbour = (right, left)

    def owner_of(s, way):
        return index_of(lax.rem(pos + n - s, n) if way == 0 else lax.rem(pos + s, n))

    piece = kdim // QIN

    def w_copy(s, q, way):
        return pltpu.make_async_remote_copy(
            src_ref=wbuf.at[s, way, pl.ds(q * piece, piece)],
            dst_ref=wbuf.at[s + 1, way, pl.ds(q * piece, piece)],
            send_sem=ws_sem.at[s, q, way],
            recv_sem=wr_sem.at[s, q, way],
            device_id={"sp": neighbour[way]},
            device_id_type=MESH,
        )

    opiece = obuf.shape[2] // QOUT

    def o_copy(s, q, way):
        return pltpu.make_async_remote_copy(
            src_ref=obuf.at[s, way, pl.ds(q * opiece, opiece)],
            dst_ref=obuf.at[s + 1, way, pl.ds(q * opiece, opiece)],
            send_sem=os_sem.at[s, q, way],
            recv_sem=or_sem.at[s, q, way],
            device_id={"sp": neighbour[way]},
            device_id_type=MESH,
        )

    def forward(s):
        for q in range(QIN):
            for way in range(2):

                @pl.when(s > 0)
                def _():
                    w_copy(s - 1, q, way).wait_recv()

                @pl.when(s < n - 1)
                def _():
                    w_copy(s, q, way).start()

    def o_forward(s):
        for q in range(QOUT):
            for way in range(2):

                @pl.when(s > 0)
                def _():
                    o_copy(s - 1, q, way).wait_recv()

                @pl.when(s < n - 1)
                def _():
                    o_copy(s, q, way).start()

    own_at = pl.multiple_of(HALO + tp * rows, HALO)
    x = tokens[...].astype(f32)
    x = x * lax.rsqrt(jnp.mean(x * x, axis=1, keepdims=True) + epsilon)
    norm[pl.ds(own_at, rows), :] = (x * in_scale[...].astype(f32)).astype(bf16)
    acc[...] = jnp.zeros_like(acc)

    for copy in local_copies:
        copy.wait()
    pl.semaphore_wait(barrier, n - 1 + T - 1)

    forward(0)

    def t_copy(d):
        return pltpu.make_async_remote_copy(
            src_ref=norm.at[pl.ds(own_at, rows)],
            dst_ref=norm.at[pl.ds(own_at, rows)],
            send_sem=ts_sem.at[d],
            recv_sem=tr_sem.at[d],
            device_id={"tp": lax.rem(tp + d, T)},
            device_id_type=MESH,
        )

    for d in range(1, T):
        t_copy(d).start()

    mid = n_half - 1

    def ahead(s, carry):
        forward(s)
        return carry

    lax.fori_loop(1, max(mid, 1), ahead, 0)

    def t_wait(d):
        source = pl.multiple_of(HALO + lax.rem(tp + T - d, T) * rows, HALO)
        pltpu.make_async_remote_copy(
            src_ref=norm.at[pl.ds(source, rows)],
            dst_ref=norm.at[pl.ds(source, rows)],
            send_sem=ts_sem.at[d],
            recv_sem=tr_sem.at[d],
            device_id={"tp": lax.rem(tp + d, T)},
            device_id_type=MESH,
        ).wait_recv()

    for d in range(1, T):
        t_wait(d)

    def h_copy():
        return pltpu.make_async_remote_copy(
            src_ref=norm.at[pl.ds(length, HALO)],
            dst_ref=norm.at[pl.ds(0, HALO)],
            send_sem=h_sem.at[0],
            recv_sem=h_sem.at[1],
            device_id={"sp": lax.rem(sp + 1, n)},
            device_id_type=MESH,
        )

    @pl.when(sp < n - 1)
    def _():
        h_copy().start()

    forward(max(mid, 1))

    @pl.when(sp > 0)
    def _():
        h_copy().wait_recv()

    @pl.when(sp == 0)
    def _():
        norm[0:HALO, :] = jnp.zeros((HALO, width), bf16)

    def project(s):
        for way in range(2):
            at = pl.multiple_of(owner_of(s, way) * kdim, kdim)
            lhs = norm[:, pl.ds(at, kdim)]
            for c in range(0, half, 256):
                acc[:, way * half + c : way * half + c + 256] += jnp.dot(
                    lhs, wbuf[s, way, :, c : c + 256], preferred_element_type=f32
                )

    start = max(mid, 1)

    def body(s, carry):
        @pl.when(s > start)
        def _():
            forward(s)

        @pl.when(s == max(n - 2, start))
        def _():
            o_forward(0)

        project(s)

        @pl.when(s - start < start)
        def _():
            project(s - start)

        return carry

    lax.fori_loop(start, n, body, 0)

    def column(ref):
        index = lax.broadcasted_iota(jnp.int32, (heads, 1), 0)
        full = jnp.full((heads, 1), ref[0], f32)
        for h in range(1, heads):
            full = jnp.where(index == h, ref[h], full)
        return full

    step = jax.nn.softplus(nt(step_w[...], norm[HALO:, :])[0:heads] + column(bias))
    logs = -step * jnp.exp(column(rate)) + spikes[...]
    r_id = lax.broadcasted_iota(jnp.int32, (CHUNK, CHUNK), 0)
    c_id = lax.broadcasted_iota(jnp.int32, (CHUNK, CHUNK), 1)
    causal = r_id >= c_id
    lower = causal.astype(f32)
    eye = (r_id == c_id).astype(f32)
    lane = lax.broadcasted_iota(jnp.int32, (1, heads_width), 1)

    def spread(columns):
        full = jnp.broadcast_to(columns[:, 0:1], (columns.shape[0], heads_width))
        for h in range(1, heads):
            full = jnp.where(lane >= h * HEAD_DIM, columns[:, h : h + 1], full)
        return full

    def taps(u, weights):
        k_taps = weights.shape[0]
        w = weights[...].astype(f32)
        total = w[k_taps - 1 : k_taps] * u[8:]
        for k in range(k_taps - 1):
            total = total + w[k : k + 1] * pltpu.roll(u, k_taps - 1 - k, 0)[8:]
        return total

    blocks = length // CHUNK
    running = jnp.zeros((STATE, heads_width), f32)
    before = jnp.zeros((1, heads_width), f32)
    at_outer, at_inner, at_value, at_ogate, at_state = (i * cdim for i in range(5))
    at_write = 5 * cdim
    at_read = at_write + STATE
    for b in range(blocks):
        t0 = b * CHUNK
        take = slice(t0 + HALO - 8, t0 + HALO + CHUNK)
        own = slice(t0 + HALO, t0 + HALO + CHUNK)

        def field(begin, size, span):
            return acc[span, begin : begin + size].astype(bf16).astype(f32)

        product = field(at_inner, cdim, take) * field(at_value, cdim, take)
        mix = field(at_outer, cdim, own) * taps(product, taps_conv)
        apart[t0 : t0 + CHUNK, 0:cdim] = mix.astype(bf16)
        xs = silu(taps(field(at_state, cdim, take), taps_in))
        wr = silu(taps(field(at_write, STATE, take), taps_wr))
        rd = silu(taps(field(at_read, STATE, take), taps_rd))
        span = slice(t0, t0 + CHUNK)
        cum = nt(lower, logs[:, span], highest)
        steps = nt(eye, step[:, span], highest)
        cum_wide = spread(cum)
        weighted = xs * spread(steps)
        xbuf[span, :] = xs
        mixbuf[span, :] = weighted.astype(bf16)
        wrbuf[span, :] = wr.astype(bf16)
        rdbuf[span, :] = rd.astype(bf16)
        cumbuf[span, :] = cum_wide
        last = cum_wide[CHUNK - 1 : CHUNK]
        scaled = (weighted * jnp.exp(last - cum_wide)).astype(bf16)
        stbuf[b] = running
        running = running * jnp.exp(last) + jnp.dot(
            wr.T.astype(bf16), scaled, preferred_element_type=f32
        )
        before = before + last
    st_send[0:STATE, :] = running.astype(bf16)
    st_send[STATE:, :] = jnp.broadcast_to(jnp.exp(before), (HALO, heads_width)).astype(bf16)

    z = lax.div(sp, 2)
    second = lax.rem(sp, 2)
    depth = n_half

    def x_copy():
        return pltpu.make_async_remote_copy(
            src_ref=st_send,
            dst_ref=st_recv,
            send_sem=x_sem.at[0],
            recv_sem=x_sem.at[1],
            device_id={"sp": sp + 1 - 2 * second},
            device_id_type=MESH,
        )

    def e_copy():
        return pltpu.make_async_remote_copy(
            src_ref=e_send,
            dst_ref=e_recv,
            send_sem=e_sem.at[0],
            recv_sem=e_sem.at[1],
            device_id={"sp": lax.rem(sp + 2, n)},
            device_id_type=MESH,
        )

    x_copy().start()
    o_next = 1

    def within(b):
        t0 = b * CHUNK
        span = slice(t0, t0 + CHUNK)
        scores = nt(rdbuf[span, :], wrbuf[span, :])
        cum_t = lax.dot_general(
            logs[:, span], lower, (((1,), (1,)), ((), ())),
            preferred_element_type=f32, precision=highest,
        )
        for pair in range(0, heads_width, 128):
            both = []
            for h in range(pair // HEAD_DIM, (pair + 128) // HEAD_DIM):
                diff = cumbuf[span, h * HEAD_DIM : h * HEAD_DIM + 1] - cum_t[h : h + 1, :]
                damped = scores * jnp.exp(jnp.where(causal, diff, -1e30))
                both.append(
                    jnp.dot(
                        damped.astype(bf16), mixbuf[span, pair : pair + 128],
                        preferred_element_type=f32,
                    )
                )
            first = lax.broadcasted_iota(jnp.int32, (1, 128), 1) < HEAD_DIM
            ybuf[span, pair : pair + 128] = jnp.where(first, both[0], both[1])

    for b in range(blocks):
        if b % 2 == 0 and o_next < n:
            o_forward(o_next)
            o_next += 1
        within(b)
    x_copy().wait_recv()
    other = st_recv[0:STATE, :].astype(f32)
    other_decay = st_recv[STATE : STATE + 1, :].astype(f32)
    own_decay = jnp.exp(before)
    is_second = jnp.broadcast_to(second, (1, heads_width)) == 1
    pair_buf[0] = jnp.where(
        is_second, other * own_decay + running, running * other_decay + other
    )
    pair_buf[1] = jnp.where(is_second, other, jnp.zeros_like(other))
    pair_decay = own_decay * other_decay
    first_decay = jnp.where(is_second, other_decay, jnp.ones_like(other_decay))

    group = (
        lax.div(lax.broadcasted_iota(jnp.int32, (heads_width, heads_width), 0), HEAD_DIM)
        == lax.div(lax.broadcasted_iota(jnp.int32, (heads_width, heads_width), 1), HEAD_DIM)
    ).astype(bf16)
    direct_wide = jnp.full((1, heads_width), direct[0], f32)
    for h in range(1, heads):
        direct_wide = jnp.where(lane >= h * HEAD_DIM, direct[h], direct_wide)

    def finish():
        before = jnp.zeros((1, heads_width), f32)
        arriving = pair_buf[1] + first_decay * pair_buf[2]
        for b in range(blocks):
            t0 = b * CHUNK
            span = slice(t0, t0 + CHUNK)
            own = slice(t0 + HALO, t0 + HALO + CHUNK)
            cum_wide = cumbuf[span, :]
            entering = (stbuf[b] + jnp.exp(before) * arriving).astype(bf16)
            before = before + cum_wide[CHUNK - 1 : CHUNK]
            head_out = (
                ybuf[span, :]
                + jnp.dot(rdbuf[span, :], entering, preferred_element_type=f32) * jnp.exp(cum_wide)
                + direct_wide * xbuf[span, :]
            )
            og = acc[own, at_ogate : at_ogate + cdim].astype(bf16).astype(f32)
            gated = head_out * silu(og)
            square = jnp.dot((gated * gated).astype(bf16), group, preferred_element_type=f32)
            normalized = gated * lax.rsqrt(square * (1.0 / HEAD_DIM) + epsilon)
            apart[span, cdim:] = (normalized * hscale[...].astype(f32)).astype(bf16)

    def link(j, carry):
        @pl.when(z == j)
        def _():
            @pl.when(j == 0)
            def _():
                pair_buf[2] = jnp.zeros_like(pair_buf[2])

            @pl.when(j > 0)
            def _():
                e_copy().wait_recv()
                pair_buf[2] = e_recv[...].astype(f32)

            @pl.when(j < depth - 1)
            def _():
                e_send[...] = (pair_buf[2] * pair_decay + pair_buf[0]).astype(bf16)
                e_copy().start()

            finish()

        @pl.when(o_next + j < n)
        def _():
            o_forward(o_next + j)

        return carry

    lax.fori_loop(0, depth, link, 0)
    o_next = min(o_next + depth, n)

    Y = T // CORES
    core = lax.rem(tp, CORES)
    chip = lax.div(tp, CORES)
    partner = chip * CORES + 1 - core
    ocols = 2 * ohalf

    def block_rows(y, c):
        return pl.ds(pl.multiple_of((y * CORES + c) * rows, rows), rows)

    def r1_copy(d, s):
        return pltpu.make_async_remote_copy(
            src_ref=part.at[s, block_rows(lax.rem(chip + d, Y), 1 - core)],
            dst_ref=r1.at[d, s],
            send_sem=r1s_sem.at[d, s],
            recv_sem=r1r_sem.at[d, s],
            device_id={"tp": partner},
            device_id_type=MESH,
        )

    def r2_copy(d, s):
        return pltpu.make_async_remote_copy(
            src_ref=p2.at[d, s],
            dst_ref=r2.at[d, s],
            send_sem=r2s_sem.at[d, s],
            recv_sem=r2r_sem.at[d, s],
            device_id={"tp": lax.rem(chip + d, Y) * CORES + core},
            device_id_type=MESH,
        )

    def reduce_far(s):
        for d in range(1, Y):
            r1_copy(d, s).wait_recv()
            mine = part[s, block_rows(lax.rem(chip + d, Y), core), :]
            p2[d, s] = (mine.astype(f32) + r1[d, s].astype(f32)).astype(bf16)
            r2_copy(d, s).start()

    def project_out(s, carry):
        @pl.when(s >= o_next)
        def _():
            o_forward(s)

        for way in range(2):
            part[s, :, way * ohalf : (way + 1) * ohalf] = jnp.dot(
                apart[...], obuf[s, way], preferred_element_type=f32
            ).astype(bf16)
        for d in range(1, Y):
            r1_copy(d, s).start()
        r1_copy(0, s).start()

        @pl.when(s > 0)
        def _():
            reduce_far(s - 1)

        return carry

    lax.fori_loop(0, n, project_out, 0)
    reduce_far(n - 1)

    def collect(s, carry):
        r1_copy(0, s).wait_recv()
        total = part[s, block_rows(chip, core), :].astype(f32) + r1[0, s].astype(f32)
        for d in range(1, Y):
            r2_copy(d, s).wait_recv()
            total = total + r2[d, s].astype(f32)
        for way in range(2):
            at = pl.multiple_of(owner_of(s, way) * ocols + way * ohalf, ohalf)
            out[:, pl.ds(at, ohalf)] = total[:, way * ohalf : (way + 1) * ohalf].astype(bf16)
        return carry

    lax.fori_loop(0, n, collect, 0)

    def w_drain(s, carry):
        for way in range(2):
            for q in range(QIN):
                w_copy(s, q, way).wait_send()
            for q in range(QOUT):
                o_copy(s, q, way).wait_send()
        return carry

    lax.fori_loop(0, n - 1, w_drain, 0)
    for d in range(1, T):
        t_copy(d).wait_send()

    @pl.when(sp < n - 1)
    def _():
        h_copy().wait_send()

    x_copy().wait_send()

    @pl.when(z < depth - 1)
    def _():
        e_copy().wait_send()

    def r_drain(s, carry):
        for d in range(Y):
            r1_copy(d, s).wait_send()
        for d in range(1, Y):
            r2_copy(d, s).wait_send()
        return carry

    lax.fori_loop(0, n, r_drain, 0)


def shifted(shard, axis, by):
    devices = lax.axis_size(axis)
    pairs = [(i, i + by) for i in range(devices) if 0 <= i + by < devices]
    return lax.ppermute(shard, axis, pairs)


def prefix(shard, axis, combine, identity):
    devices, index = (lax.axis_size(axis), lax.axis_index(axis))
    everything = jax.tree.map(
        lambda part, kind: lax.all_gather(part.astype(kind), axis),
        shard,
        (jnp.bfloat16, jnp.bfloat16),
    )
    start = jax.tree.map(
        lambda part, zero: jnp.broadcast_to(jnp.asarray(zero, part.dtype), part.shape),
        shard,
        identity,
    )

    def turn(k, before):
        reached = k < index
        new = combine(
            before, jax.tree.map(lambda part, own: part[k].astype(own.dtype), everything, shard)
        )
        return jax.tree.map(lambda a, b: jnp.where(reached, a, b), new, before)

    return lax.fori_loop(0, devices, turn, start)


def causal_taps(values, rim_rows, tap_weights):
    tap_count = tap_weights.shape[0]
    length = values.shape[0]
    padded = jnp.concatenate([rim_rows, values], axis=0)
    running = tap_weights[0] * padded[0:length]
    for offset in range(1, tap_count):
        running = running + tap_weights[offset] * padded[offset : offset + length]
    return running


def combine_states(earlier, later):
    return (earlier[0] * later[0], earlier[1] * later[0][:, None, None] + later[1])


def plain_path(
    tokens,
    input_norm_scale,
    outer_gate_weight,
    inner_gate_weight,
    value_weight_matrix,
    output_gate_weight,
    state_input_weight,
    write_key_weight,
    read_key_weight,
    step_size_weight,
    gated_conv_weight,
    input_conv_weight,
    write_conv_weight,
    read_conv_weight,
    step_size_bias,
    log_decay_rate,
    decay_spikes,
    direct_path_weight,
    head_norm_scale,
    conv_output_weight,
    state_output_weight,
):
    token_rows = tokens.astype(jnp.float32)
    scaled = token_rows * lax.rsqrt(
        jnp.mean(token_rows * token_rows, axis=1, keepdims=True) + epsilon
    )
    normed_own = (scaled * input_norm_scale.astype(jnp.float32)).astype(jnp.bfloat16)
    normed = lax.all_gather(normed_own, "tp", axis=0, tiled=True)
    length = normed.shape[0]
    pieces = (
        lax.all_gather(outer_gate_weight, "sp", axis=0, tiled=True),
        lax.all_gather(inner_gate_weight, "sp", axis=0, tiled=True),
        lax.all_gather(value_weight_matrix, "sp", axis=0, tiled=True),
        lax.all_gather(output_gate_weight, "sp", axis=0, tiled=True),
        lax.all_gather(state_input_weight, "sp", axis=0, tiled=True),
        lax.all_gather(write_key_weight, "sp", axis=0, tiled=True),
        lax.all_gather(read_key_weight, "sp", axis=0, tiled=True),
    )
    projected = tuple(
        (jnp.dot(normed, weight_rows, preferred_element_type=jnp.float32) for weight_rows in pieces)
    )
    outer_gate, inner_gate, conv_input, out_gate, state_input, write_keys, read_keys = [
        member.astype(jnp.bfloat16) for member in projected
    ]
    step_raw = jnp.dot(normed, step_size_weight, preferred_element_type=jnp.float32)
    short_rim = gated_conv_weight.shape[0] - 1
    state_rim = input_conv_weight.shape[0] - 1
    rim_rows = shifted(
        (
            inner_gate[length - short_rim :],
            conv_input[length - short_rim :],
            state_input[length - state_rim :],
            write_keys[length - state_rim :],
            read_keys[length - state_rim :],
        ),
        "sp",
        1,
    )
    product = inner_gate.astype(jnp.float32) * conv_input.astype(jnp.float32)
    rim_product = rim_rows[0].astype(jnp.float32) * rim_rows[1].astype(jnp.float32)
    mixer_part = (
        outer_gate.astype(jnp.float32)
        * causal_taps(product, rim_product, gated_conv_weight.astype(jnp.float32))
    ).astype(jnp.bfloat16)
    seq_input = jax.nn.silu(
        causal_taps(
            state_input.astype(jnp.float32),
            rim_rows[2].astype(jnp.float32),
            input_conv_weight.astype(jnp.float32),
        )
    )
    seq_write = jax.nn.silu(
        causal_taps(
            write_keys.astype(jnp.float32),
            rim_rows[3].astype(jnp.float32),
            write_conv_weight.astype(jnp.float32),
        )
    )
    seq_read = jax.nn.silu(
        causal_taps(
            read_keys.astype(jnp.float32),
            rim_rows[4].astype(jnp.float32),
            read_conv_weight.astype(jnp.float32),
        )
    )
    discrete_step = jax.nn.softplus(step_raw + step_size_bias[None, :])
    step_logarithm = discrete_step * (-jnp.exp(log_decay_rate))[None, :] + decay_spikes.T
    heads_here = discrete_step.shape[1]
    groups_here = seq_write.shape[1] // STATE
    per_group = heads_here // groups_here
    blocks = length // PLAIN_BLOCK
    input_blocks = seq_input.reshape(blocks, PLAIN_BLOCK, heads_here, HEAD_DIM)
    weighted = input_blocks * discrete_step.reshape(blocks, PLAIN_BLOCK, heads_here, 1)
    write_blocks = jnp.repeat(
        seq_write.reshape(blocks, PLAIN_BLOCK, groups_here, STATE), per_group, axis=2
    )
    read_blocks = jnp.repeat(seq_read.reshape(blocks, PLAIN_BLOCK, groups_here, STATE), per_group, axis=2)
    cumulative = jnp.cumsum(step_logarithm.reshape(blocks, PLAIN_BLOCK, heads_here), axis=1)
    causal = lax.broadcasted_iota(jnp.int32, (PLAIN_BLOCK, PLAIN_BLOCK), 0) >= lax.broadcasted_iota(
        jnp.int32, (PLAIN_BLOCK, PLAIN_BLOCK), 1
    )
    scores = jnp.einsum("clhm,cshm->clsh", read_blocks, write_blocks, precision=highest)
    damping = jnp.exp(
        jnp.where(
            causal[None, :, :, None],
            cumulative[:, :, None, :] - cumulative[:, None, :, :],
            -jnp.inf,
        )
    )
    within_block = jnp.einsum("clsh,cshp->clhp", scores * damping, weighted, precision=highest)
    to_end = jnp.exp(cumulative[:, -1:, :] - cumulative)
    block_states = jnp.einsum(
        "cshm,cshp->chpm", write_blocks * to_end[..., None], weighted, precision=highest
    )
    block_logs = cumulative[:, -1, :]

    def advance(carried_state, inputs):
        contribution, block_log = inputs
        return (carried_state * jnp.exp(block_log)[:, None, None] + contribution, carried_state)

    own_total, own_before = lax.scan(
        advance, jnp.zeros(block_states.shape[1:], jnp.float32), (block_states, block_logs)
    )
    total_log = jnp.sum(block_logs, axis=0)
    arriving = prefix(
        (jnp.exp(total_log), own_total),
        "sp",
        combine_states,
        (jnp.ones_like(total_log), jnp.zeros_like(own_total)),
    )[1]
    before_logs = jnp.cumsum(block_logs, axis=0) - block_logs
    entering = own_before + jnp.exp(before_logs)[:, :, None, None] * arriving[None]
    from_before = (
        jnp.einsum("clhm,chpm->clhp", read_blocks, entering, precision=highest)
        * jnp.exp(cumulative)[..., None]
    )
    head_out = within_block + from_before + direct_path_weight[None, None, :, None] * input_blocks
    head_out = head_out.reshape(length, heads_here * HEAD_DIM)
    gated_heads = (head_out * jax.nn.silu(out_gate.astype(jnp.float32))).reshape(
        length, heads_here, HEAD_DIM
    )
    normalized = gated_heads * lax.rsqrt(
        jnp.mean(gated_heads * gated_heads, axis=2, keepdims=True) + epsilon
    )
    state_part = (
        normalized.reshape(length, heads_here * HEAD_DIM) * head_norm_scale.astype(jnp.float32)
    ).astype(jnp.bfloat16)
    wide_mixer, wide_state = (
        lax.all_gather(conv_output_weight, "sp", axis=1, tiled=True),
        lax.all_gather(state_output_weight, "sp", axis=1, tiled=True),
    )
    return lax.psum_scatter(
        (
            jnp.dot(mixer_part, wide_mixer, preferred_element_type=jnp.float32)
            + jnp.dot(state_part, wide_state, preferred_element_type=jnp.float32)
        ).astype(jnp.bfloat16),
        "tp",
        scatter_dimension=0,
        tiled=True,
    )


def per_device(
    tokens, input_norm_scale, outer_gate_weight, inner_gate_weight, value_weight_matrix,
    output_gate_weight, state_input_weight, write_key_weight, read_key_weight, step_size_weight,
    gated_conv_weight, input_conv_weight, write_conv_weight, read_conv_weight, step_size_bias,
    log_decay_rate, decay_spikes, direct_path_weight, head_norm_scale, conv_output_weight,
    state_output_weight,
):
    n, T = lax.axis_size("sp"), lax.axis_size("tp")
    rows, width = tokens.shape
    kdim, cdim = outer_gate_weight.shape
    heads = step_size_bias.shape[0]
    hw = heads * HEAD_DIM
    half = 3 * cdim
    length = rows * T
    ocols = conv_output_weight.shape[1]
    if kdim % 128 or ocols % 256 or n % 2 or T % CORES or write_key_weight.shape[1] != STATE:
        return plain_path(
            tokens, input_norm_scale, outer_gate_weight, inner_gate_weight,
            value_weight_matrix, output_gate_weight, state_input_weight, write_key_weight,
            read_key_weight, step_size_weight, gated_conv_weight, input_conv_weight,
            write_conv_weight, read_conv_weight, step_size_bias, log_decay_rate, decay_spikes,
            direct_path_weight, head_norm_scale, conv_output_weight, state_output_weight,
        )
    Y = T // CORES
    step_w = jnp.pad(step_size_weight.T, ((0, 16 - heads), (0, 0)))
    vm = pl.BlockSpec(memory_space=pltpu.VMEM)
    sm = pl.BlockSpec(memory_space=pltpu.SMEM)
    hbm = pl.BlockSpec(memory_space=pl.ANY)
    dma = pltpu.SemaphoreType.DMA
    return pl.pallas_call(
        functools.partial(kernel, n, T),
        out_shape=jax.ShapeDtypeStruct((rows, width), bf16),
        in_specs=[vm] * 2 + [hbm] * 7 + [vm] * 5 + [sm] * 2 + [vm, sm, vm] + [hbm] * 2,
        out_specs=vm,
        scratch_shapes=[
            pltpu.VMEM((n, 2, kdim, half), bf16),
            pltpu.VMEM((n, 2, cdim + hw, ocols // 2), bf16),
            pltpu.VMEM((HALO + length, width), bf16),
            pltpu.VMEM((HALO + length, 2 * half), f32),
            pltpu.VMEM((length, hw), bf16),
            pltpu.VMEM((length, hw), f32),
            pltpu.VMEM((length, STATE), bf16),
            pltpu.VMEM((length, STATE), bf16),
            pltpu.VMEM((length, hw), f32),
            pltpu.VMEM((length, hw), f32),
            pltpu.VMEM((length // CHUNK, STATE, hw), f32),
            pltpu.VMEM((STATE + HALO, hw), bf16),
            pltpu.VMEM((STATE + HALO, hw), bf16),
            pltpu.VMEM((STATE, hw), bf16),
            pltpu.VMEM((STATE, hw), bf16),
            pltpu.VMEM((3, STATE, hw), f32),
            pltpu.VMEM((length, cdim + hw), bf16),
            pltpu.VMEM((n, length, ocols), bf16),
            pltpu.VMEM((Y, n, rows, ocols), bf16),
            pltpu.VMEM((Y, n, rows, ocols), bf16),
            pltpu.VMEM((Y, n, rows, ocols), bf16),
            dma((11,)),
            dma((n, QIN, 2)),
            dma((n, QIN, 2)),
            dma((n, QOUT, 2)),
            dma((n, QOUT, 2)),
            dma((T,)),
            dma((T,)),
            dma((2,)),
            dma((2,)),
            dma((2,)),
            dma((Y, n)),
            dma((Y, n)),
            dma((Y, n)),
            dma((Y, n)),
        ],
        compiler_params=pltpu.CompilerParams(
            collective_id=0, has_side_effects=True, vmem_limit_bytes=62 * 1024 * 1024
        ),
    )(
        tokens, input_norm_scale[None, :], outer_gate_weight, inner_gate_weight,
        value_weight_matrix, output_gate_weight, state_input_weight, write_key_weight,
        read_key_weight, step_w, gated_conv_weight, input_conv_weight, write_conv_weight,
        read_conv_weight, step_size_bias, log_decay_rate, decay_spikes, direct_path_weight,
        head_norm_scale[None, :],
        conv_output_weight, state_output_weight,
    )


def solution(mesh):
    placed = (
        (P(("sp", "tp"), None), P())
        + (P("sp", "tp"),) * 7
        + (P(None, "tp"),) * 5
        + (P("tp"), P("tp"), P("tp", "sp"), P("tp"), P("tp"), P("tp", "sp"), P("tp", "sp"))
    )
    return jax.shard_map(
        per_device, mesh=mesh, in_specs=placed, out_specs=P(("sp", "tp"), None), check_vma=False
    )
```

```python
import functools

import jax
import jax.numpy as jnp
from jax import lax
from jax.experimental import pallas as pl
from jax.experimental.pallas import tpu as pltpu
from jax.sharding import PartitionSpec as P

HEAD_DIM = 64
STATE = 128
PLAIN_BLOCK = 64
CHUNK = 128
HALO = 16
QIN = 2
QOUT = 2
CORES = 2
epsilon = 1e-05
highest = lax.Precision.HIGHEST
f32 = jnp.float32
bf16 = jnp.bfloat16
MESH = pl.DeviceIdType.MESH


def nt(a, b, precision=None):
    return lax.dot_general(
        a, b, (((1,), (1,)), ((), ())), preferred_element_type=f32, precision=precision
    )


def silu(v):
    return v / (1.0 + jnp.exp(-v))


def kernel(
    n,
    T,
    tokens,
    in_scale,
    w_outer,
    w_inner,
    w_value,
    w_ogate,
    w_state,
    w_write,
    w_read,
    step_w,
    taps_conv,
    taps_in,
    taps_wr,
    taps_rd,
    bias,
    rate,
    spikes,
    direct,
    hscale,
    o_conv,
    o_state,
    out,
    wbuf,
    obuf,
    norm,
    acc,
    mixbuf,
    xbuf,
    wrbuf,
    rdbuf,
    ybuf,
    cumbuf,
    stbuf,
    st_send,
    st_recv,
    e_send,
    e_recv,
    pair_buf,
    apart,
    part,
    r1,
    p2,
    r2,
    loc_sem,
    ws_sem,
    wr_sem,
    os_sem,
    or_sem,
    ts_sem,
    tr_sem,
    h_sem,
    x_sem,
    e_sem,
    r1s_sem,
    r1r_sem,
    r2s_sem,
    r2r_sem,
):
    sp = lax.axis_index("sp")
    tp = lax.axis_index("tp")
    rows, width = tokens.shape
    kdim = w_outer.shape[0]
    cdim = w_outer.shape[1]
    half = wbuf.shape[3]
    length = rows * T
    heads_width = xbuf.shape[1]
    heads = heads_width // HEAD_DIM
    n_half = n // 2

    barrier = pltpu.get_barrier_semaphore()
    for d in range(1, n):
        pl.semaphore_signal(
            barrier, inc=1, device_id={"sp": lax.rem(sp + d, n)}, device_id_type=MESH
        )
    for d in range(1, T):
        pl.semaphore_signal(
            barrier, inc=1, device_id={"tp": lax.rem(tp + d, T)}, device_id_type=MESH
        )

    locals_ = []
    at = 0
    for ref in (w_outer, w_inner, w_value):
        locals_.append((ref, wbuf.at[0, 0, :, at : at + ref.shape[1]]))
        at += ref.shape[1]
    at = 0
    for ref in (w_ogate, w_state, w_write, w_read):
        locals_.append((ref, wbuf.at[0, 1, :, at : at + ref.shape[1]]))
        at += ref.shape[1]
    ohalf = obuf.shape[3]
    for way in range(2):
        cut = pl.ds(way * ohalf, ohalf)
        locals_.append((o_conv.at[:, cut], obuf.at[0, way, pl.ds(0, cdim)]))
        locals_.append((o_state.at[:, cut], obuf.at[0, way, pl.ds(cdim, heads_width)]))
    local_copies = [
        pltpu.make_async_copy(src, dst, loc_sem.at[i]) for i, (src, dst) in enumerate(locals_)
    ]
    for copy in local_copies:
        copy.start()

    def pos_of(index):
        odd = lax.rem(index, 2)
        low = lax.div(index, 2)
        return (1 - odd) * low + odd * (n - 1 - low)

    def index_of(pos):
        high = lax.div(pos, n_half)
        return (1 - high) * 2 * pos + high * (2 * (n - 1 - pos) + 1)

    pos = pos_of(sp)
    right = index_of(lax.rem(pos + 1, n))
    left = index_of(lax.rem(pos + n - 1, n))
    neighbour = (right, left)

    def owner_of(s, way):
        return index_of(lax.rem(pos + n - s, n) if way == 0 else lax.rem(pos + s, n))

    piece = kdim // QIN

    def w_copy(s, q, way):
        return pltpu.make_async_remote_copy(
            src_ref=wbuf.at[s, way, pl.ds(q * piece, piece)],
            dst_ref=wbuf.at[s + 1, way, pl.ds(q * piece, piece)],
            send_sem=ws_sem.at[s, q, way],
            recv_sem=wr_sem.at[s, q, way],
            device_id={"sp": neighbour[way]},
            device_id_type=MESH,
        )

    opiece = obuf.shape[2] // QOUT

    def o_copy(s, q, way):
        return pltpu.make_async_remote_copy(
            src_ref=obuf.at[s, way, pl.ds(q * opiece, opiece)],
            dst_ref=obuf.at[s + 1, way, pl.ds(q * opiece, opiece)],
            send_sem=os_sem.at[s, q, way],
            recv_sem=or_sem.at[s, q, way],
            device_id={"sp": neighbour[way]},
            device_id_type=MESH,
        )

    def forward(s):
        for q in range(QIN):
            for way in range(2):

                @pl.when(s > 0)
                def _():
                    w_copy(s - 1, q, way).wait_recv()

                @pl.when(s < n - 1)
                def _():
                    w_copy(s, q, way).start()

    def o_forward(s):
        for q in range(QOUT):
            for way in range(2):

                @pl.when(s > 0)
                def _():
                    o_copy(s - 1, q, way).wait_recv()

                @pl.when(s < n - 1)
                def _():
                    o_copy(s, q, way).start()

    own_at = pl.multiple_of(HALO + tp * rows, HALO)
    x = tokens[...].astype(f32)
    x = x * lax.rsqrt(jnp.mean(x * x, axis=1, keepdims=True) + epsilon)
    norm[pl.ds(own_at, rows), :] = (x * in_scale[...].astype(f32).reshape(1, width)).astype(bf16)
    acc[...] = jnp.zeros_like(acc)

    for copy in local_copies:
        copy.wait()
    pl.semaphore_wait(barrier, n - 1 + T - 1)

    forward(0)

    def t_copy(d):
        return pltpu.make_async_remote_copy(
            src_ref=norm.at[pl.ds(own_at, rows)],
            dst_ref=norm.at[pl.ds(own_at, rows)],
            send_sem=ts_sem.at[d],
            recv_sem=tr_sem.at[d],
            device_id={"tp": lax.rem(tp + d, T)},
            device_id_type=MESH,
        )

    for d in range(1, T):
        t_copy(d).start()

    mid = n_half - 1

    def ahead(s, carry):
        forward(s)
        return carry

    lax.fori_loop(1, max(mid, 1), ahead, 0)

    def t_wait(d):
        source = pl.multiple_of(HALO + lax.rem(tp + T - d, T) * rows, HALO)
        pltpu.make_async_remote_copy(
            src_ref=norm.at[pl.ds(source, rows)],
            dst_ref=norm.at[pl.ds(source, rows)],
            send_sem=ts_sem.at[d],
            recv_sem=tr_sem.at[d],
            device_id={"tp": lax.rem(tp + d, T)},
            device_id_type=MESH,
        ).wait_recv()

    for d in range(1, T):
        t_wait(d)

    def h_copy():
        return pltpu.make_async_remote_copy(
            src_ref=norm.at[pl.ds(length, HALO)],
            dst_ref=norm.at[pl.ds(0, HALO)],
            send_sem=h_sem.at[0],
            recv_sem=h_sem.at[1],
            device_id={"sp": lax.rem(sp + 1, n)},
            device_id_type=MESH,
        )

    @pl.when(sp < n - 1)
    def _():
        h_copy().start()

    forward(max(mid, 1))

    @pl.when(sp > 0)
    def _():
        h_copy().wait_recv()

    @pl.when(sp == 0)
    def _():
        norm[0:HALO, :] = jnp.zeros((HALO, width), bf16)

    def project(s):
        for way in range(2):
            at = pl.multiple_of(owner_of(s, way) * kdim, kdim)
            lhs = norm[:, pl.ds(at, kdim)]
            for c in range(0, half, 256):
                acc[:, way * half + c : way * half + c + 256] += jnp.dot(
                    lhs, wbuf[s, way, :, c : c + 256], preferred_element_type=f32
                )

    start = max(mid, 1)

    def body(s, carry):
        @pl.when(s > start)
        def _():
            forward(s)

        @pl.when(s == max(n - 2, start))
        def _():
            o_forward(0)

        project(s)

        @pl.when(s - start < start)
        def _():
            project(s - start)

        return carry

    lax.fori_loop(start, n, body, 0)

    def column(ref):
        index = lax.broadcasted_iota(jnp.int32, (heads, 1), 0)
        full = jnp.full((heads, 1), ref[0], f32)
        for h in range(1, heads):
            full = jnp.where(index == h, ref[h], full)
        return full

    step = jax.nn.softplus(jnp.dot(norm[HALO:, :], step_w[...], preferred_element_type=f32).T + column(bias))
    logs = -step * jnp.exp(column(rate)) + spikes[...]
    r_id = lax.broadcasted_iota(jnp.int32, (CHUNK, CHUNK), 0)
    c_id = lax.broadcasted_iota(jnp.int32, (CHUNK, CHUNK), 1)
    causal = r_id >= c_id
    lower = causal.astype(f32)
    eye = (r_id == c_id).astype(f32)
    lane = lax.broadcasted_iota(jnp.int32, (1, heads_width), 1)

    def spread(columns):
        full = jnp.broadcast_to(columns[:, 0:1], (columns.shape[0], heads_width))
        for h in range(1, heads):
            full = jnp.where(lane >= h * HEAD_DIM, columns[:, h : h + 1], full)
        return full

    def taps(u, weights):
        k_taps = weights.shape[0]
        w = weights[...].astype(f32)
        total = w[k_taps - 1 : k_taps] * u[8:]
        for k in range(k_taps - 1):
            total = total + w[k : k + 1] * pltpu.roll(u, k_taps - 1 - k, 0)[8:]
        return total

    blocks = length // CHUNK
    running = jnp.zeros((STATE, heads_width), f32)
    before = jnp.zeros((1, heads_width), f32)
    at_outer, at_inner, at_value, at_ogate, at_state = (i * cdim for i in range(5))
    at_write = 5 * cdim
    at_read = at_write + STATE
    for b in range(blocks):
        t0 = b * CHUNK
        take = slice(t0 + HALO - 8, t0 + HALO + CHUNK)
        own = slice(t0 + HALO, t0 + HALO + CHUNK)

        def field(begin, size, span):
            return acc[span, begin : begin + size].astype(bf16).astype(f32)

        product = field(at_inner, cdim, take) * field(at_value, cdim, take)
        mix = field(at_outer, cdim, own) * taps(product, taps_conv)
        apart[t0 : t0 + CHUNK, 0:cdim] = mix.astype(bf16)
        xs = silu(taps(field(at_state, cdim, take), taps_in))
        wr = silu(taps(field(at_write, STATE, take), taps_wr))
        rd = silu(taps(field(at_read, STATE, take), taps_rd))
        span = slice(t0, t0 + CHUNK)
        cum = nt(lower, logs[:, span], highest)
        steps = nt(eye, step[:, span], highest)
        cum_wide = spread(cum)
        weighted = xs * spread(steps)
        xbuf[span, :] = xs
        mixbuf[span, :] = weighted.astype(bf16)
        wrbuf[span, :] = wr.astype(bf16)
        rdbuf[span, :] = rd.astype(bf16)
        cumbuf[span, :] = cum_wide
        last = cum_wide[CHUNK - 1 : CHUNK]
        scaled = (weighted * jnp.exp(last - cum_wide)).astype(bf16)
        stbuf[b] = running
        running = running * jnp.exp(last) + jnp.dot(
            wr.T.astype(bf16), scaled, preferred_element_type=f32
        )
        before = before + last
    st_send[0:STATE, :] = running.astype(bf16)
    st_send[STATE:, :] = jnp.broadcast_to(jnp.exp(before), (HALO, heads_width)).astype(bf16)

    z = lax.div(sp, 2)
    second = lax.rem(sp, 2)
    depth = n_half

    def x_copy():
        return pltpu.make_async_remote_copy(
            src_ref=st_send,
            dst_ref=st_recv,
            send_sem=x_sem.at[0],
            recv_sem=x_sem.at[1],
            device_id={"sp": sp + 1 - 2 * second},
            device_id_type=MESH,
        )

    def e_copy():
        return pltpu.make_async_remote_copy(
            src_ref=e_send,
            dst_ref=e_recv,
            send_sem=e_sem.at[0],
            recv_sem=e_sem.at[1],
            device_id={"sp": lax.rem(sp + 2, n)},
            device_id_type=MESH,
        )

    x_copy().start()
    o_next = 1

    def within(b):
        t0 = b * CHUNK
        span = slice(t0, t0 + CHUNK)
        scores = nt(rdbuf[span, :], wrbuf[span, :])
        cum_t = lax.dot_general(
            logs[:, span], lower, (((1,), (1,)), ((), ())),
            preferred_element_type=f32, precision=highest,
        )
        for pair in range(0, heads_width, 128):
            both = []
            for h in range(pair // HEAD_DIM, (pair + 128) // HEAD_DIM):
                diff = cumbuf[span, h * HEAD_DIM : h * HEAD_DIM + 1] - cum_t[h : h + 1, :]
                damped = scores * jnp.exp(jnp.where(causal, diff, -1e30))
                both.append(
                    jnp.dot(
                        damped.astype(bf16), mixbuf[span, pair : pair + 128],
                        preferred_element_type=f32,
                    )
                )
            first = lax.broadcasted_iota(jnp.int32, (1, 128), 1) < HEAD_DIM
            ybuf[span, pair : pair + 128] = jnp.where(first, both[0], both[1])

    for b in range(blocks):
        if b % 2 == 0 and o_next < n:
            o_forward(o_next)
            o_next += 1
        within(b)
    x_copy().wait_recv()
    other = st_recv[0:STATE, :].astype(f32)
    other_decay = st_recv[STATE : STATE + 1, :].astype(f32)
    own_decay = jnp.exp(before)
    is_second = jnp.broadcast_to(second, (1, heads_width)) == 1
    pair_buf[0] = jnp.where(
        is_second, other * own_decay + running, running * other_decay + other
    )
    pair_buf[1] = jnp.where(is_second, other, jnp.zeros_like(other))
    pair_decay = own_decay * other_decay
    first_decay = jnp.where(is_second, other_decay, jnp.ones_like(other_decay))

    group = (
        lax.div(lax.broadcasted_iota(jnp.int32, (heads_width, heads_width), 0), HEAD_DIM)
        == lax.div(lax.broadcasted_iota(jnp.int32, (heads_width, heads_width), 1), HEAD_DIM)
    ).astype(bf16)
    direct_wide = jnp.full((1, heads_width), direct[0], f32)
    for h in range(1, heads):
        direct_wide = jnp.where(lane >= h * HEAD_DIM, direct[h], direct_wide)

    def finish():
        before = jnp.zeros((1, heads_width), f32)
        arriving = pair_buf[1] + first_decay * pair_buf[2]
        for b in range(blocks):
            t0 = b * CHUNK
            span = slice(t0, t0 + CHUNK)
            own = slice(t0 + HALO, t0 + HALO + CHUNK)
            cum_wide = cumbuf[span, :]
            entering = (stbuf[b] + jnp.exp(before) * arriving).astype(bf16)
            before = before + cum_wide[CHUNK - 1 : CHUNK]
            head_out = (
                ybuf[span, :]
                + jnp.dot(rdbuf[span, :], entering, preferred_element_type=f32) * jnp.exp(cum_wide)
                + direct_wide * xbuf[span, :]
            )
            og = acc[own, at_ogate : at_ogate + cdim].astype(bf16).astype(f32)
            gated = head_out * silu(og)
            square = jnp.dot((gated * gated).astype(bf16), group, preferred_element_type=f32)
            normalized = gated * lax.rsqrt(square * (1.0 / HEAD_DIM) + epsilon)
            apart[span, cdim:] = (normalized * hscale[...].astype(f32).reshape(1, heads_width)).astype(bf16)

    Y = T // CORES
    core = lax.rem(tp, CORES)
    chip = lax.div(tp, CORES)
    partner = chip * CORES + 1 - core
    ocols = 2 * ohalf

    def block_rows(y, c):
        return pl.ds(pl.multiple_of((y * CORES + c) * rows, rows), rows)

    def r1_copy(d, s):
        return pltpu.make_async_remote_copy(
            src_ref=part.at[s, block_rows(lax.rem(chip + d, Y), 1 - core)],
            dst_ref=r1.at[d, s],
            send_sem=r1s_sem.at[d, s],
            recv_sem=r1r_sem.at[d, s],
            device_id={"tp": partner},
            device_id_type=MESH,
        )

    def r2_copy(d, s):
        return pltpu.make_async_remote_copy(
            src_ref=p2.at[d, s],
            dst_ref=r2.at[d, s],
            send_sem=r2s_sem.at[d, s],
            recv_sem=r2r_sem.at[d, s],
            device_id={"tp": lax.rem(chip + d, Y) * CORES + core},
            device_id_type=MESH,
        )

    def reduce_far(s):
        for d in range(1, Y):
            r1_copy(d, s).wait_recv()
            mine = part[s, block_rows(lax.rem(chip + d, Y), core), :]
            p2[d, s] = (mine.astype(f32) + r1[d, s].astype(f32)).astype(bf16)
            r2_copy(d, s).start()

    def project_out(s, carry):
        for way in range(2):
            part[s, :, way * ohalf : (way + 1) * ohalf] = jnp.dot(
                apart[...], obuf[s, way], preferred_element_type=f32
            ).astype(bf16)
        for d in range(1, Y):
            r1_copy(d, s).start()
        r1_copy(0, s).start()

        @pl.when(s > 0)
        def _():
            reduce_far(s - 1)

        return carry

    def link(j, carry):
        @pl.when(z == j)
        def _():
            @pl.when(j == 0)
            def _():
                pair_buf[2] = jnp.zeros_like(pair_buf[2])

            @pl.when(j > 0)
            def _():
                e_copy().wait_recv()
                pair_buf[2] = e_recv[...].astype(f32)

            @pl.when(j < depth - 1)
            def _():
                e_send[...] = (pair_buf[2] * pair_decay + pair_buf[0]).astype(bf16)
                e_copy().start()

            finish()
            lax.fori_loop(0, o_next + j, project_out, 0)

        @pl.when(o_next + j < n)
        def _():
            o_forward(o_next + j)

            @pl.when(z <= j)
            def _():
                project_out(o_next + j, 0)

        return carry

    lax.fori_loop(0, depth, link, 0)

    def rest(s, carry):
        o_forward(s)
        project_out(s, 0)
        return carry

    lax.fori_loop(min(o_next + depth, n), n, rest, 0)
    reduce_far(n - 1)

    def collect(s, carry):
        r1_copy(0, s).wait_recv()
        total = part[s, block_rows(chip, core), :].astype(f32) + r1[0, s].astype(f32)
        for d in range(1, Y):
            r2_copy(d, s).wait_recv()
            total = total + r2[d, s].astype(f32)
        for way in range(2):
            at = pl.multiple_of(owner_of(s, way) * ocols + way * ohalf, ohalf)
            out[:, pl.ds(at, ohalf)] = total[:, way * ohalf : (way + 1) * ohalf].astype(bf16)
        return carry

    lax.fori_loop(0, n, collect, 0)

    def w_drain(s, carry):
        for way in range(2):
            for q in range(QIN):
                w_copy(s, q, way).wait_send()
            for q in range(QOUT):
                o_copy(s, q, way).wait_send()
        return carry

    lax.fori_loop(0, n - 1, w_drain, 0)
    for d in range(1, T):
        t_copy(d).wait_send()

    @pl.when(sp < n - 1)
    def _():
        h_copy().wait_send()

    x_copy().wait_send()

    @pl.when(z < depth - 1)
    def _():
        e_copy().wait_send()

    def r_drain(s, carry):
        for d in range(Y):
            r1_copy(d, s).wait_send()
        for d in range(1, Y):
            r2_copy(d, s).wait_send()
        return carry

    lax.fori_loop(0, n, r_drain, 0)


def shifted(shard, axis, by):
    devices = lax.axis_size(axis)
    pairs = [(i, i + by) for i in range(devices) if 0 <= i + by < devices]
    return lax.ppermute(shard, axis, pairs)


def prefix(shard, axis, combine, identity):
    devices, index = (lax.axis_size(axis), lax.axis_index(axis))
    everything = jax.tree.map(
        lambda part, kind: lax.all_gather(part.astype(kind), axis),
        shard,
        (jnp.bfloat16, jnp.bfloat16),
    )
    start = jax.tree.map(
        lambda part, zero: jnp.broadcast_to(jnp.asarray(zero, part.dtype), part.shape),
        shard,
        identity,
    )

    def turn(k, before):
        reached = k < index
        new = combine(
            before, jax.tree.map(lambda part, own: part[k].astype(own.dtype), everything, shard)
        )
        return jax.tree.map(lambda a, b: jnp.where(reached, a, b), new, before)

    return lax.fori_loop(0, devices, turn, start)


def causal_taps(values, rim_rows, tap_weights):
    tap_count = tap_weights.shape[0]
    length = values.shape[0]
    padded = jnp.concatenate([rim_rows, values], axis=0)
    running = tap_weights[0] * padded[0:length]
    for offset in range(1, tap_count):
        running = running + tap_weights[offset] * padded[offset : offset + length]
    return running


def combine_states(earlier, later):
    return (earlier[0] * later[0], earlier[1] * later[0][:, None, None] + later[1])


def plain_path(
    tokens,
    input_norm_scale,
    outer_gate_weight,
    inner_gate_weight,
    value_weight_matrix,
    output_gate_weight,
    state_input_weight,
    write_key_weight,
    read_key_weight,
    step_size_weight,
    gated_conv_weight,
    input_conv_weight,
    write_conv_weight,
    read_conv_weight,
    step_size_bias,
    log_decay_rate,
    decay_spikes,
    direct_path_weight,
    head_norm_scale,
    conv_output_weight,
    state_output_weight,
):
    token_rows = tokens.astype(jnp.float32)
    scaled = token_rows * lax.rsqrt(
        jnp.mean(token_rows * token_rows, axis=1, keepdims=True) + epsilon
    )
    normed_own = (scaled * input_norm_scale.astype(jnp.float32)).astype(jnp.bfloat16)
    normed = lax.all_gather(normed_own, "tp", axis=0, tiled=True)
    length = normed.shape[0]
    pieces = (
        lax.all_gather(outer_gate_weight, "sp", axis=0, tiled=True),
        lax.all_gather(inner_gate_weight, "sp", axis=0, tiled=True),
        lax.all_gather(value_weight_matrix, "sp", axis=0, tiled=True),
        lax.all_gather(output_gate_weight, "sp", axis=0, tiled=True),
        lax.all_gather(state_input_weight, "sp", axis=0, tiled=True),
        lax.all_gather(write_key_weight, "sp", axis=0, tiled=True),
        lax.all_gather(read_key_weight, "sp", axis=0, tiled=True),
    )
    projected = tuple(
        (jnp.dot(normed, weight_rows, preferred_element_type=jnp.float32) for weight_rows in pieces)
    )
    outer_gate, inner_gate, conv_input, out_gate, state_input, write_keys, read_keys = [
        member.astype(jnp.bfloat16) for member in projected
    ]
    step_raw = jnp.dot(normed, step_size_weight, preferred_element_type=jnp.float32)
    short_rim = gated_conv_weight.shape[0] - 1
    state_rim = input_conv_weight.shape[0] - 1
    rim_rows = shifted(
        (
            inner_gate[length - short_rim :],
            conv_input[length - short_rim :],
            state_input[length - state_rim :],
            write_keys[length - state_rim :],
            read_keys[length - state_rim :],
        ),
        "sp",
        1,
    )
    product = inner_gate.astype(jnp.float32) * conv_input.astype(jnp.float32)
    rim_product = rim_rows[0].astype(jnp.float32) * rim_rows[1].astype(jnp.float32)
    mixer_part = (
        outer_gate.astype(jnp.float32)
        * causal_taps(product, rim_product, gated_conv_weight.astype(jnp.float32))
    ).astype(jnp.bfloat16)
    seq_input = jax.nn.silu(
        causal_taps(
            state_input.astype(jnp.float32),
            rim_rows[2].astype(jnp.float32),
            input_conv_weight.astype(jnp.float32),
        )
    )
    seq_write = jax.nn.silu(
        causal_taps(
            write_keys.astype(jnp.float32),
            rim_rows[3].astype(jnp.float32),
            write_conv_weight.astype(jnp.float32),
        )
    )
    seq_read = jax.nn.silu(
        causal_taps(
            read_keys.astype(jnp.float32),
            rim_rows[4].astype(jnp.float32),
            read_conv_weight.astype(jnp.float32),
        )
    )
    discrete_step = jax.nn.softplus(step_raw + step_size_bias[None, :])
    step_logarithm = discrete_step * (-jnp.exp(log_decay_rate))[None, :] + decay_spikes.T
    heads_here = discrete_step.shape[1]
    groups_here = seq_write.shape[1] // STATE
    per_group = heads_here // groups_here
    blocks = length // PLAIN_BLOCK
    input_blocks = seq_input.reshape(blocks, PLAIN_BLOCK, heads_here, HEAD_DIM)
    weighted = input_blocks * discrete_step.reshape(blocks, PLAIN_BLOCK, heads_here, 1)
    write_blocks = jnp.repeat(
        seq_write.reshape(blocks, PLAIN_BLOCK, groups_here, STATE), per_group, axis=2
    )
    read_blocks = jnp.repeat(seq_read.reshape(blocks, PLAIN_BLOCK, groups_here, STATE), per_group, axis=2)
    cumulative = jnp.cumsum(step_logarithm.reshape(blocks, PLAIN_BLOCK, heads_here), axis=1)
    causal = lax.broadcasted_iota(jnp.int32, (PLAIN_BLOCK, PLAIN_BLOCK), 0) >= lax.broadcasted_iota(
        jnp.int32, (PLAIN_BLOCK, PLAIN_BLOCK), 1
    )
    scores = jnp.einsum("clhm,cshm->clsh", read_blocks, write_blocks, precision=highest)
    damping = jnp.exp(
        jnp.where(
            causal[None, :, :, None],
            cumulative[:, :, None, :] - cumulative[:, None, :, :],
            -jnp.inf,
        )
    )
    within_block = jnp.einsum("clsh,cshp->clhp", scores * damping, weighted, precision=highest)
    to_end = jnp.exp(cumulative[:, -1:, :] - cumulative)
    block_states = jnp.einsum(
        "cshm,cshp->chpm", write_blocks * to_end[..., None], weighted, precision=highest
    )
    block_logs = cumulative[:, -1, :]

    def advance(carried_state, inputs):
        contribution, block_log = inputs
        return (carried_state * jnp.exp(block_log)[:, None, None] + contribution, carried_state)

    own_total, own_before = lax.scan(
        advance, jnp.zeros(block_states.shape[1:], jnp.float32), (block_states, block_logs)
    )
    total_log = jnp.sum(block_logs, axis=0)
    arriving = prefix(
        (jnp.exp(total_log), own_total),
        "sp",
        combine_states,
        (jnp.ones_like(total_log), jnp.zeros_like(own_total)),
    )[1]
    before_logs = jnp.cumsum(block_logs, axis=0) - block_logs
    entering = own_before + jnp.exp(before_logs)[:, :, None, None] * arriving[None]
    from_before = (
        jnp.einsum("clhm,chpm->clhp", read_blocks, entering, precision=highest)
        * jnp.exp(cumulative)[..., None]
    )
    head_out = within_block + from_before + direct_path_weight[None, None, :, None] * input_blocks
    head_out = head_out.reshape(length, heads_here * HEAD_DIM)
    gated_heads = (head_out * jax.nn.silu(out_gate.astype(jnp.float32))).reshape(
        length, heads_here, HEAD_DIM
    )
    normalized = gated_heads * lax.rsqrt(
        jnp.mean(gated_heads * gated_heads, axis=2, keepdims=True) + epsilon
    )
    state_part = (
        normalized.reshape(length, heads_here * HEAD_DIM) * head_norm_scale.astype(jnp.float32)
    ).astype(jnp.bfloat16)
    wide_mixer, wide_state = (
        lax.all_gather(conv_output_weight, "sp", axis=1, tiled=True),
        lax.all_gather(state_output_weight, "sp", axis=1, tiled=True),
    )
    return lax.psum_scatter(
        (
            jnp.dot(mixer_part, wide_mixer, preferred_element_type=jnp.float32)
            + jnp.dot(state_part, wide_state, preferred_element_type=jnp.float32)
        ).astype(jnp.bfloat16),
        "tp",
        scatter_dimension=0,
        tiled=True,
    )


def per_device(
    tokens, input_norm_scale, outer_gate_weight, inner_gate_weight, value_weight_matrix,
    output_gate_weight, state_input_weight, write_key_weight, read_key_weight, step_size_weight,
    gated_conv_weight, input_conv_weight, write_conv_weight, read_conv_weight, step_size_bias,
    log_decay_rate, decay_spikes, direct_path_weight, head_norm_scale, conv_output_weight,
    state_output_weight,
):
    n, T = lax.axis_size("sp"), lax.axis_size("tp")
    rows, width = tokens.shape
    kdim, cdim = outer_gate_weight.shape
    heads = step_size_bias.shape[0]
    hw = heads * HEAD_DIM
    half = 3 * cdim
    length = rows * T
    ocols = conv_output_weight.shape[1]
    if kdim % 128 or ocols % 256 or n % 2 or T % CORES or write_key_weight.shape[1] != STATE:
        return plain_path(
            tokens, input_norm_scale, outer_gate_weight, inner_gate_weight,
            value_weight_matrix, output_gate_weight, state_input_weight, write_key_weight,
            read_key_weight, step_size_weight, gated_conv_weight, input_conv_weight,
            write_conv_weight, read_conv_weight, step_size_bias, log_decay_rate, decay_spikes,
            direct_path_weight, head_norm_scale, conv_output_weight, state_output_weight,
        )
    Y = T // CORES
    vm = pl.BlockSpec(memory_space=pltpu.VMEM)
    sm = pl.BlockSpec(memory_space=pltpu.SMEM)
    hbm = pl.BlockSpec(memory_space=pl.ANY)
    dma = pltpu.SemaphoreType.DMA
    return pl.pallas_call(
        functools.partial(kernel, n, T),
        out_shape=jax.ShapeDtypeStruct((rows, width), bf16),
        in_specs=[vm] * 2 + [hbm] * 7 + [vm] * 5 + [sm] * 2 + [vm, sm, vm] + [hbm] * 2,
        out_specs=vm,
        scratch_shapes=[
            pltpu.VMEM((n, 2, kdim, half), bf16),
            pltpu.VMEM((n, 2, cdim + hw, ocols // 2), bf16),
            pltpu.VMEM((HALO + length, width), bf16),
            pltpu.VMEM((HALO + length, 2 * half), f32),
            pltpu.VMEM((length, hw), bf16),
            pltpu.VMEM((length, hw), f32),
            pltpu.VMEM((length, STATE), bf16),
            pltpu.VMEM((length, STATE), bf16),
            pltpu.VMEM((length, hw), f32),
            pltpu.VMEM((length, hw), f32),
            pltpu.VMEM((length // CHUNK, STATE, hw), f32),
            pltpu.VMEM((STATE + HALO, hw), bf16),
            pltpu.VMEM((STATE + HALO, hw), bf16),
            pltpu.VMEM((STATE, hw), bf16),
            pltpu.VMEM((STATE, hw), bf16),
            pltpu.VMEM((3, STATE, hw), f32),
            pltpu.VMEM((length, cdim + hw), bf16),
            pltpu.VMEM((n, length, ocols), bf16),
            pltpu.VMEM((Y, n, rows, ocols), bf16),
            pltpu.VMEM((Y, n, rows, ocols), bf16),
            pltpu.VMEM((Y, n, rows, ocols), bf16),
            dma((11,)),
            dma((n, QIN, 2)),
            dma((n, QIN, 2)),
            dma((n, QOUT, 2)),
            dma((n, QOUT, 2)),
            dma((T,)),
            dma((T,)),
            dma((2,)),
            dma((2,)),
            dma((2,)),
            dma((Y, n)),
            dma((Y, n)),
            dma((Y, n)),
            dma((Y, n)),
        ],
        compiler_params=pltpu.CompilerParams(
            collective_id=0, has_side_effects=True, vmem_limit_bytes=62 * 1024 * 1024
        ),
    )(
        tokens, input_norm_scale, outer_gate_weight, inner_gate_weight,
        value_weight_matrix, output_gate_weight, state_input_weight, write_key_weight,
        read_key_weight, step_size_weight, gated_conv_weight, input_conv_weight, write_conv_weight,
        read_conv_weight, step_size_bias, log_decay_rate, decay_spikes, direct_path_weight,
        head_norm_scale,
        conv_output_weight, state_output_weight,
    )


def solution(mesh):
    placed = (
        (P(("sp", "tp"), None), P())
        + (P("sp", "tp"),) * 7
        + (P(None, "tp"),) * 5
        + (P("tp"), P("tp"), P("tp", "sp"), P("tp"), P("tp"), P("tp", "sp"), P("tp", "sp"))
    )
    return jax.shard_map(
        per_device, mesh=mesh, in_specs=placed, out_specs=P(("sp", "tp"), None), check_vma=False
    )
```

```python
import functools

import jax
import jax.numpy as jnp
from jax import lax
from jax.experimental import pallas as pl
from jax.experimental.pallas import tpu as pltpu
from jax.sharding import PartitionSpec as P

HEAD_DIM = 64
STATE = 128
PLAIN_BLOCK = 64
CHUNK = 128
HALO = 16
QIN = 2
QOUT = 2
CORES = 2
epsilon = 1e-05
highest = lax.Precision.HIGHEST
f32 = jnp.float32
bf16 = jnp.bfloat16
MESH = pl.DeviceIdType.MESH


def nt(a, b, precision=None):
    return lax.dot_general(
        a, b, (((1,), (1,)), ((), ())), preferred_element_type=f32, precision=precision
    )


def silu(v):
    return v / (1.0 + jnp.exp(-v))


def kernel(
    n,
    T,
    tokens,
    in_scale,
    w_outer,
    w_inner,
    w_value,
    w_ogate,
    w_state,
    w_write,
    w_read,
    step_w,
    taps_conv,
    taps_in,
    taps_wr,
    taps_rd,
    bias,
    rate,
    spikes,
    direct,
    hscale,
    o_conv,
    o_state,
    out,
    wbuf,
    obuf,
    norm,
    acc,
    mixbuf,
    xbuf,
    wrbuf,
    rdbuf,
    ybuf,
    cumbuf,
    stbuf,
    st_send,
    st_recv,
    e_send,
    e_recv,
    pair_buf,
    apart,
    part,
    r1,
    p2,
    r2,
    loc_sem,
    ws_sem,
    wr_sem,
    os_sem,
    or_sem,
    ts_sem,
    tr_sem,
    h_sem,
    x_sem,
    e_sem,
    r1s_sem,
    r1r_sem,
    r2s_sem,
    r2r_sem,
):
    sp = lax.axis_index("sp")
    tp = lax.axis_index("tp")
    rows, width = tokens.shape
    kdim = w_outer.shape[0]
    cdim = w_outer.shape[1]
    half = wbuf.shape[3]
    length = rows * T
    heads_width = xbuf.shape[1]
    heads = heads_width // HEAD_DIM
    n_half = n // 2

    barrier = pltpu.get_barrier_semaphore()
    for d in range(1, n):
        pl.semaphore_signal(
            barrier, inc=1, device_id={"sp": lax.rem(sp + d, n)}, device_id_type=MESH
        )
    for d in range(1, T):
        pl.semaphore_signal(
            barrier, inc=1, device_id={"tp": lax.rem(tp + d, T)}, device_id_type=MESH
        )

    locals_ = []
    at = 0
    for ref in (w_outer, w_inner, w_value):
        locals_.append((ref, wbuf.at[0, 0, :, at : at + ref.shape[1]]))
        at += ref.shape[1]
    at = 0
    for ref in (w_ogate, w_state, w_write, w_read):
        locals_.append((ref, wbuf.at[0, 1, :, at : at + ref.shape[1]]))
        at += ref.shape[1]
    ohalf = obuf.shape[3]
    for way in range(2):
        cut = pl.ds(way * ohalf, ohalf)
        locals_.append((o_conv.at[:, cut], obuf.at[0, way, pl.ds(0, cdim)]))
        locals_.append((o_state.at[:, cut], obuf.at[0, way, pl.ds(cdim, heads_width)]))
    local_copies = [
        pltpu.make_async_copy(src, dst, loc_sem.at[i]) for i, (src, dst) in enumerate(locals_)
    ]
    for copy in local_copies:
        copy.start()

    def pos_of(index):
        odd = lax.rem(index, 2)
        low = lax.div(index, 2)
        return (1 - odd) * low + odd * (n - 1 - low)

    def index_of(pos):
        high = lax.div(pos, n_half)
        return (1 - high) * 2 * pos + high * (2 * (n - 1 - pos) + 1)

    pos = pos_of(sp)
    right = index_of(lax.rem(pos + 1, n))
    left = index_of(lax.rem(pos + n - 1, n))
    neighbour = (right, left)

    def owner_of(s, way):
        return index_of(lax.rem(pos + n - s, n) if way == 0 else lax.rem(pos + s, n))

    piece = kdim // QIN

    def w_copy(s, q, way):
        return pltpu.make_async_remote_copy(
            src_ref=wbuf.at[s, way, pl.ds(q * piece, piece)],
            dst_ref=wbuf.at[s + 1, way, pl.ds(q * piece, piece)],
            send_sem=ws_sem.at[s, q, way],
            recv_sem=wr_sem.at[s, q, way],
            device_id={"sp": neighbour[way]},
            device_id_type=MESH,
        )

    opiece = obuf.shape[2] // QOUT

    def o_copy(s, q, way):
        return pltpu.make_async_remote_copy(
            src_ref=obuf.at[s, way, pl.ds(q * opiece, opiece)],
            dst_ref=obuf.at[s + 1, way, pl.ds(q * opiece, opiece)],
            send_sem=os_sem.at[s, q, way],
            recv_sem=or_sem.at[s, q, way],
            device_id={"sp": neighbour[way]},
            device_id_type=MESH,
        )

    def forward(s):
        for q in range(QIN):
            for way in range(2):

                @pl.when(s > 0)
                def _():
                    w_copy(s - 1, q, way).wait_recv()

                @pl.when(s < n - 1)
                def _():
                    w_copy(s, q, way).start()

    def o_forward(s):
        for q in range(QOUT):
            for way in range(2):

                @pl.when(s > 0)
                def _():
                    o_copy(s - 1, q, way).wait_recv()

                @pl.when(s < n - 1)
                def _():
                    o_copy(s, q, way).start()

    own_at = pl.multiple_of(HALO + tp * rows, HALO)
    x = tokens[...].astype(f32)
    x = x * lax.rsqrt(jnp.mean(x * x, axis=1, keepdims=True) + epsilon)
    norm[pl.ds(own_at, rows), :] = (x * in_scale[...].astype(f32).reshape(1, width)).astype(bf16)
    acc[...] = jnp.zeros_like(acc)

    for copy in local_copies:
        copy.wait()
    pl.semaphore_wait(barrier, n - 1 + T - 1)

    forward(0)

    def t_copy(d):
        return pltpu.make_async_remote_copy(
            src_ref=norm.at[pl.ds(own_at, rows)],
            dst_ref=norm.at[pl.ds(own_at, rows)],
            send_sem=ts_sem.at[d],
            recv_sem=tr_sem.at[d],
            device_id={"tp": lax.rem(tp + d, T)},
            device_id_type=MESH,
        )

    for d in range(1, T):
        t_copy(d).start()

    mid = n_half - 1

    def ahead(s, carry):
        forward(s)
        return carry

    lax.fori_loop(1, max(mid, 1), ahead, 0)

    def t_wait(d):
        source = pl.multiple_of(HALO + lax.rem(tp + T - d, T) * rows, HALO)
        pltpu.make_async_remote_copy(
            src_ref=norm.at[pl.ds(source, rows)],
            dst_ref=norm.at[pl.ds(source, rows)],
            send_sem=ts_sem.at[d],
            recv_sem=tr_sem.at[d],
            device_id={"tp": lax.rem(tp + d, T)},
            device_id_type=MESH,
        ).wait_recv()

    for d in range(1, T):
        t_wait(d)

    def h_copy():
        return pltpu.make_async_remote_copy(
            src_ref=norm.at[pl.ds(length, HALO)],
            dst_ref=norm.at[pl.ds(0, HALO)],
            send_sem=h_sem.at[0],
            recv_sem=h_sem.at[1],
            device_id={"sp": lax.rem(sp + 1, n)},
            device_id_type=MESH,
        )

    @pl.when(sp < n - 1)
    def _():
        h_copy().start()

    forward(max(mid, 1))

    @pl.when(sp > 0)
    def _():
        h_copy().wait_recv()

    @pl.when(sp == 0)
    def _():
        norm[0:HALO, :] = jnp.zeros((HALO, width), bf16)

    def project(s):
        for way in range(2):
            at = pl.multiple_of(owner_of(s, way) * kdim, kdim)
            lhs = norm[:, pl.ds(at, kdim)]
            for c in range(0, half, 256):
                acc[:, way * half + c : way * half + c + 256] += jnp.dot(
                    lhs, wbuf[s, way, :, c : c + 256], preferred_element_type=f32
                )

    start = max(mid, 1)

    def body(s, carry):
        @pl.when(s > start)
        def _():
            forward(s)

        @pl.when(s == max(n - 2, start))
        def _():
            o_forward(0)

        project(s)

        @pl.when(s - start < start)
        def _():
            project(s - start)

        return carry

    lax.fori_loop(start, n, body, 0)

    def column(ref):
        index = lax.broadcasted_iota(jnp.int32, (heads, 1), 0)
        full = jnp.full((heads, 1), ref[0], f32)
        for h in range(1, heads):
            full = jnp.where(index == h, ref[h], full)
        return full

    step = jax.nn.softplus(jnp.dot(norm[HALO:, :], step_w[...], preferred_element_type=f32).T + column(bias))
    logs = -step * jnp.exp(column(rate)) + spikes[...]
    r_id = lax.broadcasted_iota(jnp.int32, (CHUNK, CHUNK), 0)
    c_id = lax.broadcasted_iota(jnp.int32, (CHUNK, CHUNK), 1)
    causal = r_id >= c_id
    lower = causal.astype(f32)
    eye = (r_id == c_id).astype(f32)
    lane = lax.broadcasted_iota(jnp.int32, (1, heads_width), 1)

    def spread(columns):
        full = jnp.broadcast_to(columns[:, 0:1], (columns.shape[0], heads_width))
        for h in range(1, heads):
            full = jnp.where(lane >= h * HEAD_DIM, columns[:, h : h + 1], full)
        return full

    def taps(u, weights):
        k_taps = weights.shape[0]
        w = weights[...].astype(f32)
        total = w[k_taps - 1 : k_taps] * u[8:]
        for k in range(k_taps - 1):
            total = total + w[k : k + 1] * pltpu.roll(u, k_taps - 1 - k, 0)[8:]
        return total

    blocks = length // CHUNK
    running = jnp.zeros((STATE, heads_width), f32)
    before = jnp.zeros((1, heads_width), f32)
    at_outer, at_inner, at_value, at_ogate, at_state = (i * cdim for i in range(5))
    at_write = 5 * cdim
    at_read = at_write + STATE
    for b in range(blocks):
        t0 = b * CHUNK
        take = slice(t0 + HALO - 8, t0 + HALO + CHUNK)
        own = slice(t0 + HALO, t0 + HALO + CHUNK)

        def field(begin, size, span):
            return acc[span, begin : begin + size].astype(bf16).astype(f32)

        product = field(at_inner, cdim, take) * field(at_value, cdim, take)
        mix = field(at_outer, cdim, own) * taps(product, taps_conv)
        apart[t0 : t0 + CHUNK, 0:cdim] = mix.astype(bf16)
        xs = silu(taps(field(at_state, cdim, take), taps_in))
        wr = silu(taps(field(at_write, STATE, take), taps_wr))
        rd = silu(taps(field(at_read, STATE, take), taps_rd))
        span = slice(t0, t0 + CHUNK)
        cum = nt(lower, logs[:, span], highest)
        steps = nt(eye, step[:, span], highest)
        cum_wide = spread(cum)
        weighted = xs * spread(steps)
        xbuf[span, :] = xs
        mixbuf[span, :] = weighted.astype(bf16)
        wrbuf[span, :] = wr.astype(bf16)
        rdbuf[span, :] = rd.astype(bf16)
        cumbuf[span, :] = cum_wide
        last = cum_wide[CHUNK - 1 : CHUNK]
        scaled = (weighted * jnp.exp(last - cum_wide)).astype(bf16)
        stbuf[b] = running
        running = running * jnp.exp(last) + jnp.dot(
            wr.T.astype(bf16), scaled, preferred_element_type=f32
        )
        before = before + last
    st_send[0:STATE, :] = running.astype(bf16)
    st_send[STATE:, :] = jnp.broadcast_to(jnp.exp(before), (HALO, heads_width)).astype(bf16)

    z = lax.div(sp, 2)
    second = lax.rem(sp, 2)
    depth = n_half

    def x_copy():
        return pltpu.make_async_remote_copy(
            src_ref=st_send,
            dst_ref=st_recv,
            send_sem=x_sem.at[0],
            recv_sem=x_sem.at[1],
            device_id={"sp": sp + 1 - 2 * second},
            device_id_type=MESH,
        )

    def e_copy():
        return pltpu.make_async_remote_copy(
            src_ref=e_send,
            dst_ref=e_recv,
            send_sem=e_sem.at[0],
            recv_sem=e_sem.at[1],
            device_id={"sp": lax.rem(sp + 2, n)},
            device_id_type=MESH,
        )

    x_copy().start()
    o_next = 1

    def within(b):
        t0 = b * CHUNK
        span = slice(t0, t0 + CHUNK)
        scores = nt(rdbuf[span, :], wrbuf[span, :])
        cum_t = lax.dot_general(
            logs[:, span], lower, (((1,), (1,)), ((), ())),
            preferred_element_type=f32, precision=highest,
        )
        for pair in range(0, heads_width, 128):
            both = []
            for h in range(pair // HEAD_DIM, (pair + 128) // HEAD_DIM):
                diff = cumbuf[span, h * HEAD_DIM : h * HEAD_DIM + 1] - cum_t[h : h + 1, :]
                damped = scores * jnp.exp(jnp.where(causal, diff, -1e30))
                both.append(
                    jnp.dot(
                        damped.astype(bf16), mixbuf[span, pair : pair + 128],
                        preferred_element_type=f32,
                    )
                )
            first = lax.broadcasted_iota(jnp.int32, (1, 128), 1) < HEAD_DIM
            ybuf[span, pair : pair + 128] = jnp.where(first, both[0], both[1])

    for b in range(blocks):
        if b % 2 == 0 and o_next < n:
            o_forward(o_next)
            o_next += 1
        within(b)
    x_copy().wait_recv()
    other = st_recv[0:STATE, :].astype(f32)
    other_decay = st_recv[STATE : STATE + 1, :].astype(f32)
    own_decay = jnp.exp(before)
    is_second = jnp.broadcast_to(second, (1, heads_width)) == 1
    pair_buf[0] = jnp.where(
        is_second, other * own_decay + running, running * other_decay + other
    )
    pair_buf[1] = jnp.where(is_second, other, jnp.zeros_like(other))
    pair_decay = own_decay * other_decay
    first_decay = jnp.where(is_second, other_decay, jnp.ones_like(other_decay))

    group = (
        lax.div(lax.broadcasted_iota(jnp.int32, (heads_width, heads_width), 0), HEAD_DIM)
        == lax.div(lax.broadcasted_iota(jnp.int32, (heads_width, heads_width), 1), HEAD_DIM)
    ).astype(bf16)
    direct_wide = jnp.full((1, heads_width), direct[0], f32)
    for h in range(1, heads):
        direct_wide = jnp.where(lane >= h * HEAD_DIM, direct[h], direct_wide)

    def finish():
        before = jnp.zeros((1, heads_width), f32)
        arriving = pair_buf[1] + first_decay * pair_buf[2]
        for b in range(blocks):
            t0 = b * CHUNK
            span = slice(t0, t0 + CHUNK)
            own = slice(t0 + HALO, t0 + HALO + CHUNK)
            cum_wide = cumbuf[span, :]
            entering = (stbuf[b] + jnp.exp(before) * arriving).astype(bf16)
            before = before + cum_wide[CHUNK - 1 : CHUNK]
            head_out = (
                ybuf[span, :]
                + jnp.dot(rdbuf[span, :], entering, preferred_element_type=f32) * jnp.exp(cum_wide)
                + direct_wide * xbuf[span, :]
            )
            og = acc[own, at_ogate : at_ogate + cdim].astype(bf16).astype(f32)
            gated = head_out * silu(og)
            square = jnp.dot((gated * gated).astype(bf16), group, preferred_element_type=f32)
            normalized = gated * lax.rsqrt(square * (1.0 / HEAD_DIM) + epsilon)
            apart[span, cdim:] = (normalized * hscale[...].astype(f32).reshape(1, heads_width)).astype(bf16)

    Y = T // CORES
    core = lax.rem(tp, CORES)
    chip = lax.div(tp, CORES)
    partner = chip * CORES + 1 - core
    ocols = 2 * ohalf

    def block_rows(y, c):
        return pl.ds(pl.multiple_of((y * CORES + c) * rows, rows), rows)

    def r1_copy(d, s):
        return pltpu.make_async_remote_copy(
            src_ref=part.at[s, block_rows(lax.rem(chip + d, Y), 1 - core)],
            dst_ref=r1.at[d, s],
            send_sem=r1s_sem.at[d, s],
            recv_sem=r1r_sem.at[d, s],
            device_id={"tp": partner},
            device_id_type=MESH,
        )

    def r2_copy(d, s):
        return pltpu.make_async_remote_copy(
            src_ref=p2.at[d, s],
            dst_ref=r2.at[d, s],
            send_sem=r2s_sem.at[d, s],
            recv_sem=r2r_sem.at[d, s],
            device_id={"tp": lax.rem(chip + d, Y) * CORES + core},
            device_id_type=MESH,
        )

    def reduce_far(s):
        for d in range(1, Y):
            r1_copy(d, s).wait_recv()
            mine = part[s, block_rows(lax.rem(chip + d, Y), core), :]
            p2[d, s] = (mine.astype(f32) + r1[d, s].astype(f32)).astype(bf16)
            r2_copy(d, s).start()

    def project_out(s, carry):
        for way in range(2):
            part[s, :, way * ohalf : (way + 1) * ohalf] = jnp.dot(
                apart[...], obuf[s, way], preferred_element_type=f32
            ).astype(bf16)
        for d in range(1, Y):
            r1_copy(d, s).start()
        r1_copy(0, s).start()

        @pl.when(s > 0)
        def _():
            reduce_far(s - 1)

        return carry

    def link(j, carry):
        @pl.when(z == j)
        def _():
            @pl.when(j == 0)
            def _():
                pair_buf[2] = jnp.zeros_like(pair_buf[2])

            @pl.when(j > 0)
            def _():
                e_copy().wait_recv()
                pair_buf[2] = e_recv[...].astype(f32)

            @pl.when(j < depth - 1)
            def _():
                e_send[...] = (pair_buf[2] * pair_decay + pair_buf[0]).astype(bf16)
                e_copy().start()

            finish()

        @pl.when(o_next + j < n)
        def _():
            o_forward(o_next + j)

            @pl.when(z < j)
            def _():
                project_out(o_next + j, 0)

            @pl.when(z == j)
            def _():
                lax.fori_loop(0, o_next + j + 1, project_out, 0)

        return carry

    lax.fori_loop(0, depth, link, 0)

    def rest(s, carry):
        o_forward(s)
        project_out(s, 0)
        return carry

    lax.fori_loop(min(o_next + depth, n), n, rest, 0)
    reduce_far(n - 1)

    def collect(s, carry):
        r1_copy(0, s).wait_recv()
        total = part[s, block_rows(chip, core), :].astype(f32) + r1[0, s].astype(f32)
        for d in range(1, Y):
            r2_copy(d, s).wait_recv()
            total = total + r2[d, s].astype(f32)
        for way in range(2):
            at = pl.multiple_of(owner_of(s, way) * ocols + way * ohalf, ohalf)
            out[:, pl.ds(at, ohalf)] = total[:, way * ohalf : (way + 1) * ohalf].astype(bf16)
        return carry

    lax.fori_loop(0, n, collect, 0)

    def w_drain(s, carry):
        for way in range(2):
            for q in range(QIN):
                w_copy(s, q, way).wait_send()
            for q in range(QOUT):
                o_copy(s, q, way).wait_send()
        return carry

    lax.fori_loop(0, n - 1, w_drain, 0)
    for d in range(1, T):
        t_copy(d).wait_send()

    @pl.when(sp < n - 1)
    def _():
        h_copy().wait_send()

    x_copy().wait_send()

    @pl.when(z < depth - 1)
    def _():
        e_copy().wait_send()

    def r_drain(s, carry):
        for d in range(Y):
            r1_copy(d, s).wait_send()
        for d in range(1, Y):
            r2_copy(d, s).wait_send()
        return carry

    lax.fori_loop(0, n, r_drain, 0)


def shifted(shard, axis, by):
    devices = lax.axis_size(axis)
    pairs = [(i, i + by) for i in range(devices) if 0 <= i + by < devices]
    return lax.ppermute(shard, axis, pairs)


def prefix(shard, axis, combine, identity):
    devices, index = (lax.axis_size(axis), lax.axis_index(axis))
    everything = jax.tree.map(
        lambda part, kind: lax.all_gather(part.astype(kind), axis),
        shard,
        (jnp.bfloat16, jnp.bfloat16),
    )
    start = jax.tree.map(
        lambda part, zero: jnp.broadcast_to(jnp.asarray(zero, part.dtype), part.shape),
        shard,
        identity,
    )

    def turn(k, before):
        reached = k < index
        new = combine(
            before, jax.tree.map(lambda part, own: part[k].astype(own.dtype), everything, shard)
        )
        return jax.tree.map(lambda a, b: jnp.where(reached, a, b), new, before)

    return lax.fori_loop(0, devices, turn, start)


def causal_taps(values, rim_rows, tap_weights):
    tap_count = tap_weights.shape[0]
    length = values.shape[0]
    padded = jnp.concatenate([rim_rows, values], axis=0)
    running = tap_weights[0] * padded[0:length]
    for offset in range(1, tap_count):
        running = running + tap_weights[offset] * padded[offset : offset + length]
    return running


def combine_states(earlier, later):
    return (earlier[0] * later[0], earlier[1] * later[0][:, None, None] + later[1])


def plain_path(
    tokens,
    input_norm_scale,
    outer_gate_weight,
    inner_gate_weight,
    value_weight_matrix,
    output_gate_weight,
    state_input_weight,
    write_key_weight,
    read_key_weight,
    step_size_weight,
    gated_conv_weight,
    input_conv_weight,
    write_conv_weight,
    read_conv_weight,
    step_size_bias,
    log_decay_rate,
    decay_spikes,
    direct_path_weight,
    head_norm_scale,
    conv_output_weight,
    state_output_weight,
):
    token_rows = tokens.astype(jnp.float32)
    scaled = token_rows * lax.rsqrt(
        jnp.mean(token_rows * token_rows, axis=1, keepdims=True) + epsilon
    )
    normed_own = (scaled * input_norm_scale.astype(jnp.float32)).astype(jnp.bfloat16)
    normed = lax.all_gather(normed_own, "tp", axis=0, tiled=True)
    length = normed.shape[0]
    pieces = (
        lax.all_gather(outer_gate_weight, "sp", axis=0, tiled=True),
        lax.all_gather(inner_gate_weight, "sp", axis=0, tiled=True),
        lax.all_gather(value_weight_matrix, "sp", axis=0, tiled=True),
        lax.all_gather(output_gate_weight, "sp", axis=0, tiled=True),
        lax.all_gather(state_input_weight, "sp", axis=0, tiled=True),
        lax.all_gather(write_key_weight, "sp", axis=0, tiled=True),
        lax.all_gather(read_key_weight, "sp", axis=0, tiled=True),
    )
    projected = tuple(
        (jnp.dot(normed, weight_rows, preferred_element_type=jnp.float32) for weight_rows in pieces)
    )
    outer_gate, inner_gate, conv_input, out_gate, state_input, write_keys, read_keys = [
        member.astype(jnp.bfloat16) for member in projected
    ]
    step_raw = jnp.dot(normed, step_size_weight, preferred_element_type=jnp.float32)
    short_rim = gated_conv_weight.shape[0] - 1
    state_rim = input_conv_weight.shape[0] - 1
    rim_rows = shifted(
        (
            inner_gate[length - short_rim :],
            conv_input[length - short_rim :],
            state_input[length - state_rim :],
            write_keys[length - state_rim :],
            read_keys[length - state_rim :],
        ),
        "sp",
        1,
    )
    product = inner_gate.astype(jnp.float32) * conv_input.astype(jnp.float32)
    rim_product = rim_rows[0].astype(jnp.float32) * rim_rows[1].astype(jnp.float32)
    mixer_part = (
        outer_gate.astype(jnp.float32)
        * causal_taps(product, rim_product, gated_conv_weight.astype(jnp.float32))
    ).astype(jnp.bfloat16)
    seq_input = jax.nn.silu(
        causal_taps(
            state_input.astype(jnp.float32),
            rim_rows[2].astype(jnp.float32),
            input_conv_weight.astype(jnp.float32),
        )
    )
    seq_write = jax.nn.silu(
        causal_taps(
            write_keys.astype(jnp.float32),
            rim_rows[3].astype(jnp.float32),
            write_conv_weight.astype(jnp.float32),
        )
    )
    seq_read = jax.nn.silu(
        causal_taps(
            read_keys.astype(jnp.float32),
            rim_rows[4].astype(jnp.float32),
            read_conv_weight.astype(jnp.float32),
        )
    )
    discrete_step = jax.nn.softplus(step_raw + step_size_bias[None, :])
    step_logarithm = discrete_step * (-jnp.exp(log_decay_rate))[None, :] + decay_spikes.T
    heads_here = discrete_step.shape[1]
    groups_here = seq_write.shape[1] // STATE
    per_group = heads_here // groups_here
    blocks = length // PLAIN_BLOCK
    input_blocks = seq_input.reshape(blocks, PLAIN_BLOCK, heads_here, HEAD_DIM)
    weighted = input_blocks * discrete_step.reshape(blocks, PLAIN_BLOCK, heads_here, 1)
    write_blocks = jnp.repeat(
        seq_write.reshape(blocks, PLAIN_BLOCK, groups_here, STATE), per_group, axis=2
    )
    read_blocks = jnp.repeat(seq_read.reshape(blocks, PLAIN_BLOCK, groups_here, STATE), per_group, axis=2)
    cumulative = jnp.cumsum(step_logarithm.reshape(blocks, PLAIN_BLOCK, heads_here), axis=1)
    causal = lax.broadcasted_iota(jnp.int32, (PLAIN_BLOCK, PLAIN_BLOCK), 0) >= lax.broadcasted_iota(
        jnp.int32, (PLAIN_BLOCK, PLAIN_BLOCK), 1
    )
    scores = jnp.einsum("clhm,cshm->clsh", read_blocks, write_blocks, precision=highest)
    damping = jnp.exp(
        jnp.where(
            causal[None, :, :, None],
            cumulative[:, :, None, :] - cumulative[:, None, :, :],
            -jnp.inf,
        )
    )
    within_block = jnp.einsum("clsh,cshp->clhp", scores * damping, weighted, precision=highest)
    to_end = jnp.exp(cumulative[:, -1:, :] - cumulative)
    block_states = jnp.einsum(
        "cshm,cshp->chpm", write_blocks * to_end[..., None], weighted, precision=highest
    )
    block_logs = cumulative[:, -1, :]

    def advance(carried_state, inputs):
        contribution, block_log = inputs
        return (carried_state * jnp.exp(block_log)[:, None, None] + contribution, carried_state)

    own_total, own_before = lax.scan(
        advance, jnp.zeros(block_states.shape[1:], jnp.float32), (block_states, block_logs)
    )
    total_log = jnp.sum(block_logs, axis=0)
    arriving = prefix(
        (jnp.exp(total_log), own_total),
        "sp",
        combine_states,
        (jnp.ones_like(total_log), jnp.zeros_like(own_total)),
    )[1]
    before_logs = jnp.cumsum(block_logs, axis=0) - block_logs
    entering = own_before + jnp.exp(before_logs)[:, :, None, None] * arriving[None]
    from_before = (
        jnp.einsum("clhm,chpm->clhp", read_blocks, entering, precision=highest)
        * jnp.exp(cumulative)[..., None]
    )
    head_out = within_block + from_before + direct_path_weight[None, None, :, None] * input_blocks
    head_out = head_out.reshape(length, heads_here * HEAD_DIM)
    gated_heads = (head_out * jax.nn.silu(out_gate.astype(jnp.float32))).reshape(
        length, heads_here, HEAD_DIM
    )
    normalized = gated_heads * lax.rsqrt(
        jnp.mean(gated_heads * gated_heads, axis=2, keepdims=True) + epsilon
    )
    state_part = (
        normalized.reshape(length, heads_here * HEAD_DIM) * head_norm_scale.astype(jnp.float32)
    ).astype(jnp.bfloat16)
    wide_mixer, wide_state = (
        lax.all_gather(conv_output_weight, "sp", axis=1, tiled=True),
        lax.all_gather(state_output_weight, "sp", axis=1, tiled=True),
    )
    return lax.psum_scatter(
        (
            jnp.dot(mixer_part, wide_mixer, preferred_element_type=jnp.float32)
            + jnp.dot(state_part, wide_state, preferred_element_type=jnp.float32)
        ).astype(jnp.bfloat16),
        "tp",
        scatter_dimension=0,
        tiled=True,
    )


def per_device(
    tokens, input_norm_scale, outer_gate_weight, inner_gate_weight, value_weight_matrix,
    output_gate_weight, state_input_weight, write_key_weight, read_key_weight, step_size_weight,
    gated_conv_weight, input_conv_weight, write_conv_weight, read_conv_weight, step_size_bias,
    log_decay_rate, decay_spikes, direct_path_weight, head_norm_scale, conv_output_weight,
    state_output_weight,
):
    n, T = lax.axis_size("sp"), lax.axis_size("tp")
    rows, width = tokens.shape
    kdim, cdim = outer_gate_weight.shape
    heads = step_size_bias.shape[0]
    hw = heads * HEAD_DIM
    half = 3 * cdim
    length = rows * T
    ocols = conv_output_weight.shape[1]
    if kdim % 128 or ocols % 256 or n % 2 or n < 6 or T % CORES or write_key_weight.shape[1] != STATE:
        return plain_path(
            tokens, input_norm_scale, outer_gate_weight, inner_gate_weight,
            value_weight_matrix, output_gate_weight, state_input_weight, write_key_weight,
            read_key_weight, step_size_weight, gated_conv_weight, input_conv_weight,
            write_conv_weight, read_conv_weight, step_size_bias, log_decay_rate, decay_spikes,
            direct_path_weight, head_norm_scale, conv_output_weight, state_output_weight,
        )
    Y = T // CORES
    vm = pl.BlockSpec(memory_space=pltpu.VMEM)
    sm = pl.BlockSpec(memory_space=pltpu.SMEM)
    hbm = pl.BlockSpec(memory_space=pl.ANY)
    dma = pltpu.SemaphoreType.DMA
    return pl.pallas_call(
        functools.partial(kernel, n, T),
        out_shape=jax.ShapeDtypeStruct((rows, width), bf16),
        in_specs=[vm] * 2 + [hbm] * 7 + [vm] * 5 + [sm] * 2 + [vm, sm, vm] + [hbm] * 2,
        out_specs=vm,
        scratch_shapes=[
            pltpu.VMEM((n, 2, kdim, half), bf16),
            pltpu.VMEM((n, 2, cdim + hw, ocols // 2), bf16),
            pltpu.VMEM((HALO + length, width), bf16),
            pltpu.VMEM((HALO + length, 2 * half), f32),
            pltpu.VMEM((length, hw), bf16),
            pltpu.VMEM((length, hw), f32),
            pltpu.VMEM((length, STATE), bf16),
            pltpu.VMEM((length, STATE), bf16),
            pltpu.VMEM((length, hw), f32),
            pltpu.VMEM((length, hw), f32),
            pltpu.VMEM((length // CHUNK, STATE, hw), f32),
            pltpu.VMEM((STATE + HALO, hw), bf16),
            pltpu.VMEM((STATE + HALO, hw), bf16),
            pltpu.VMEM((STATE, hw), bf16),
            pltpu.VMEM((STATE, hw), bf16),
            pltpu.VMEM((3, STATE, hw), f32),
            pltpu.VMEM((length, cdim + hw), bf16),
            pltpu.VMEM((n, length, ocols), bf16),
            pltpu.VMEM((Y, n, rows, ocols), bf16),
            pltpu.VMEM((Y, n, rows, ocols), bf16),
            pltpu.VMEM((Y, n, rows, ocols), bf16),
            dma((11,)),
            dma((n, QIN, 2)),
            dma((n, QIN, 2)),
            dma((n, QOUT, 2)),
            dma((n, QOUT, 2)),
            dma((T,)),
            dma((T,)),
            dma((2,)),
            dma((2,)),
            dma((2,)),
            dma((Y, n)),
            dma((Y, n)),
            dma((Y, n)),
            dma((Y, n)),
        ],
        compiler_params=pltpu.CompilerParams(
            collective_id=0, has_side_effects=True, vmem_limit_bytes=62 * 1024 * 1024
        ),
    )(
        tokens, input_norm_scale, outer_gate_weight, inner_gate_weight,
        value_weight_matrix, output_gate_weight, state_input_weight, write_key_weight,
        read_key_weight, step_size_weight, gated_conv_weight, input_conv_weight, write_conv_weight,
        read_conv_weight, step_size_bias, log_decay_rate, decay_spikes, direct_path_weight,
        head_norm_scale,
        conv_output_weight, state_output_weight,
    )


def solution(mesh):
    placed = (
        (P(("sp", "tp"), None), P())
        + (P("sp", "tp"),) * 7
        + (P(None, "tp"),) * 5
        + (P("tp"), P("tp"), P("tp", "sp"), P("tp"), P("tp"), P("tp", "sp"), P("tp", "sp"))
    )
    return jax.shard_map(
        per_device, mesh=mesh, in_specs=placed, out_specs=P(("sp", "tp"), None), check_vma=False
    )
```
